32 devices in a mesh: grp: 2 (over y), sp: 4 (over z), tp: 4 (over x, core).
Axes of the slice: x: 2, y: 2, z: 4, core: 2. Of those that a mesh axis runs over, the one named last changes fastest.
Arguments:
- conv_input: bfloat16 [4096, 1024], P(('grp', 'sp'), 'tp'), parts along dimension 0, may hold values from -6 to 6
- pre_gate: bfloat16 [4096, 1024], P(('grp', 'sp'), 'tp'), parts along dimension 0, may hold values from -6 to 6
- post_gate: bfloat16 [4096, 1024], P(('grp', 'sp'), 'tp'), parts along dimension 0, may hold values from -6 to 6
- conv_taps: float32 [3, 1024], replicated, may hold values from -3.5 to 3.5
- out_proj: bfloat16 [1024, 2048], replicated, may hold values from -0.1875 to 0.1875
- residual_in: bfloat16 [4096, 2048], P(('grp', 'sp', 'tp')), parts along dimension 0, may hold values from -6 to 6
- norm_gain: float32 [2048], replicated, may hold values from 0.1 to 1.9
- routes: int32 [4096, 2], P(('grp', 'sp', 'tp')), parts along dimension 0, may hold values from 0 to 7, as said below
- route_weight: float32 [4096, 2], P(('grp', 'sp', 'tp')), parts along dimension 0, may hold values from 0.1 to 1
- w_gate: bfloat16 [8, 2048, 1024], P('sp', None, 'tp'), may hold values from -0.125 to 0.125
- w_up: bfloat16 [8, 2048, 1024], P('sp', None, 'tp'), may hold values from -0.125 to 0.125
- w_down: bfloat16 [8, 1024, 2048], P('sp', 'tp'), may hold values from -0.1875 to 0.1875
Outputs:
- layer_out: bfloat16 [4096, 2048], P(('grp', 'sp', 'tp')), parts along dimension 0
The draws below stay inside these ranges and needn't reach their ends.
There are 2 independent parts, one for each index of `grp`. The reference program is written for one: setup_inputs(seed, part) draws one part's arguments, and reference() takes and returns one part's arrays. A program takes and returns all parts, laid end to end along the dimension named above; an argument that names none is the same for every part. Nothing has to cross between parts.
Inputs may be any that keep to these rules, and one draw needn't show every extreme that they name: `routes`: the two numbers of a row differ and lie in the same group of 2 consecutive experts. In each aligned block of 128 rows every expert is named exactly 32 times.
All inputs are finite; a program needn't handle non-finite values.
Results may differ from the reference program's by a relative error of at most 0.0085.
Values may be sent and summed in bfloat16 or wider, within the bound.
A program may use at most 64 MiB of HBM per device.

```python
import jax
import jax.numpy as jnp
from jax import lax

D = 2048
CH = 1024
HID = 1024
CONV = 3
GROUPS = 4
TOKENS = 2048
EXPERTS = 8
EPG = 2
ROW_BLOCK = 128
BLOCKS = 16
N_TP = 4


def draw_routes(key, part):
    base = jax.random.fold_in(key, 7)
    perm_key, shift_key = jax.random.split(base)
    block_keys = jax.random.split(perm_key, BLOCKS)
    ranks = jax.vmap(lambda k: jax.random.permutation(k, ROW_BLOCK))(block_keys).astype(jnp.int32)
    offsets = jax.random.randint(shift_key, (BLOCKS, 1), 0, EPG // 2).astype(jnp.int32)
    group = ranks % GROUPS
    within = ranks // GROUPS
    first = 2 * within % EPG
    second = (2 * within + 1 + 2 * offsets) % EPG
    chosen = jnp.stack([group * EPG + first, group * EPG + second], axis=-1)
    return chosen.reshape(TOKENS, 2).astype(jnp.int32)


def block_scale(own_key, shape, cuts, least, high):
    level = 1.0
    for position, shards_of in cuts:
        steps = jax.random.uniform(jax.random.fold_in(jax.random.fold_in(own_key, 6), position), (shards_of,), jnp.float32, least / len(cuts), high / len(cuts))
        level = level * jnp.repeat(jnp.exp(steps), shape[position] // shards_of).reshape((-1,) + (1,) * (len(shape) - 1 - position))
    return level


def gaussian(rng, dims, spread, most, pieces=(), held_as=jnp.bfloat16):
    entries = spread * jax.random.normal(rng, dims, jnp.float32)
    if pieces:
        entries = entries * block_scale(rng, dims, pieces, -0.22, 0.18)
    return jnp.clip(entries, -most, most).astype(held_as)


def setup_inputs(seed: int = 0, part: int = 0) -> dict:
    key_of = jax.random.split(jax.random.key(seed), 13)
    part_splits = jax.random.split(jax.random.fold_in(key_of[12], part), 13)
    conv_input = gaussian(part_splits[0], (TOKENS, CH), 1.0, 6.0, ((0, 4), (1, 4)))
    pre_gate = gaussian(part_splits[1], (TOKENS, CH), 1.0, 6.0, ((0, 4), (1, 4)))
    post_gate = gaussian(part_splits[2], (TOKENS, CH), 1.0, 6.0, ((0, 4), (1, 4)))
    conv_taps = gaussian(key_of[3], (CONV, CH), CONV ** -0.5, 3.5, (), jnp.float32)
    out_proj = gaussian(key_of[4], (CH, D), CH ** -0.5, 0.1875)
    residual_in = gaussian(part_splits[5], (TOKENS, D), 1.0, 6.0, ((0, 16),))
    norm_gain = jnp.clip(1.0 + 0.18 * jax.random.normal(key_of[6], (D,), jnp.float32), 0.1, 1.9)
    routes = draw_routes(jax.random.fold_in(jax.random.fold_in(key_of[12], part), 71), part)
    route_weight = jnp.clip(0.1 + 0.9 * jax.random.uniform(part_splits[8], (TOKENS, 2), jnp.float32) ** block_scale(part_splits[8], (TOKENS, 2), ((0, 16),), -0.2, 0.2), 0.1, 1.0)
    w_gate = gaussian(key_of[9], (EXPERTS, D, HID), D ** -0.5, 0.125, ((0, 4), (2, 4)))
    w_up = gaussian(key_of[10], (EXPERTS, D, HID), D ** -0.5, 0.125, ((0, 4), (2, 4)))
    w_down = gaussian(key_of[11], (EXPERTS, HID, D), HID ** -0.5, 0.1875, ((0, 4), (1, 4)))
    return dict(conv_input=conv_input, pre_gate=pre_gate, post_gate=post_gate, conv_taps=conv_taps, out_proj=out_proj, residual_in=residual_in, norm_gain=norm_gain, routes=routes, route_weight=route_weight, w_gate=w_gate, w_up=w_up, w_down=w_down)


def reference(conv_input, pre_gate, post_gate, conv_taps, out_proj, residual_in, norm_gain, routes, route_weight, w_gate, w_up, w_down):
    gated = pre_gate.astype(jnp.float32) * conv_input.astype(jnp.float32)
    padded = jnp.pad(gated, ((2, 0), (0, 0)))
    conv = padded[2:] * conv_taps[2] + padded[1:-1] * conv_taps[1] + padded[:-2] * conv_taps[0]
    mixed = (post_gate.astype(jnp.float32) * conv).astype(jnp.bfloat16)
    projected = jnp.dot(mixed, out_proj, preferred_element_type=jnp.float32)
    stream = residual_in.astype(jnp.float32) + projected
    scale = lax.rsqrt(lax.optimization_barrier(jnp.mean(stream * stream, axis=-1, keepdims=True)) + 1e-06)
    normed = (stream * scale * norm_gain).astype(jnp.bfloat16)
    flat_routes = routes.reshape(-1)
    per_expert = TOKENS * 2 // EXPERTS
    hid_shard = HID // N_TP

    def one_expert(carry, expert):
        picked = jnp.nonzero(flat_routes == expert, size=per_expert)[0].astype(jnp.int32)
        rows = normed[picked // 2]
        gate_all = w_gate[expert]
        up_all = w_up[expert]
        down_all = w_down[expert]
        total = jnp.zeros((per_expert, D), jnp.float32)
        for shard in range(N_TP):
            low = shard * hid_shard
            gate = jnp.dot(rows, gate_all[:, low:low + hid_shard], preferred_element_type=jnp.float32)
            upper = jnp.dot(rows, up_all[:, low:low + hid_shard], preferred_element_type=jnp.float32)
            hidden = (jax.nn.silu(gate) * upper).astype(jnp.bfloat16)
            part = jnp.dot(hidden, down_all[low:low + hid_shard], preferred_element_type=jnp.float32).astype(jnp.bfloat16)
            part = lax.optimization_barrier(part)
            total = total + part.astype(jnp.float32)
        carry = carry.at[picked].set(total.astype(jnp.bfloat16))
        return (carry, None)
    start = jnp.zeros((TOKENS * 2, D), jnp.bfloat16)
    outputs, _ = lax.scan(one_expert, start, jnp.arange(EXPERTS, dtype=jnp.int32))
    expert_out = outputs.reshape(TOKENS, 2, D).astype(jnp.float32)
    weighted = lax.optimization_barrier(jnp.sum(route_weight[:, :, None] * expert_out, axis=1))
    return (stream + weighted).astype(jnp.bfloat16)
```

```python
import functools

import jax
import jax.numpy as jnp
from jax import lax
from jax.experimental import pallas as pl
from jax.experimental.pallas import tpu as pltpu
from jax.sharding import PartitionSpec as P

GROUPS = 4
LANES = 128
F32, BF16 = jnp.float32, jnp.bfloat16


def shifted(block, axis, distance):
    devices = range(lax.axis_size(axis))
    route = [(i - distance, i) for i in devices if i - distance in devices]
    return lax.ppermute(block, axis, route)


def generic(
    conv_input,
    pre_gate,
    post_gate,
    conv_taps,
    out_proj,
    residual_in,
    norm_gain,
    routes,
    route_weight,
    w_gate,
    w_up,
    w_down,
):
    shards = lax.axis_size("tp")
    place = lax.axis_index("tp")
    seq_ranks = lax.axis_size("sp")
    channels = conv_input.shape[1]
    width = residual_in.shape[1]
    taps = lax.dynamic_slice_in_dim(conv_taps, place * channels, channels, 1)
    prior_input, prior_gate = shifted((conv_input[-2:], pre_gate[-2:]), "sp", 1)
    gated = jnp.concatenate(
        [
            prior_gate.astype(jnp.float32) * prior_input.astype(jnp.float32),
            pre_gate.astype(jnp.float32) * conv_input.astype(jnp.float32),
        ],
        axis=0,
    )
    conv = gated[2:] * taps[2] + gated[1:-1] * taps[1] + gated[:-2] * taps[0]
    mixed = (post_gate.astype(jnp.float32) * conv).astype(jnp.bfloat16)
    token_rows = lax.all_to_all(mixed, "tp", split_axis=0, concat_axis=1, tiled=True)
    projected = jnp.dot(token_rows, out_proj, preferred_element_type=jnp.float32)
    stream = residual_in.astype(jnp.float32) + projected
    scale = lax.rsqrt(jnp.mean(stream * stream, axis=-1, keepdims=True) + 1e-06)
    normed = (stream * scale * norm_gain).astype(jnp.bfloat16)
    block_rows = routes.shape[0]
    local_experts = w_gate.shape[0]
    experts = local_experts * seq_ranks
    capacity = 2 * block_rows // experts
    flat_routes = routes.reshape(-1)
    position = jnp.arange(flat_routes.shape[0], dtype=jnp.int32)
    earlier = (flat_routes[:, None] == flat_routes[None, :]) & (
        position[None, :] < position[:, None]
    )
    rank = jnp.sum(earlier.astype(jnp.int32), axis=1)
    slot = flat_routes * capacity + rank
    outgoing = (
        jnp.zeros((experts * capacity, width), jnp.bfloat16).at[slot].set(normed[position // 2])
    )
    outgoing = outgoing.reshape(seq_ranks, local_experts, capacity, width)
    spread = lax.all_gather(
        lax.all_to_all(outgoing, "sp", split_axis=0, concat_axis=0, tiled=True)[:, None],
        "tp",
        axis=1,
        tiled=True,
    )
    count = spread.shape[3]
    partials = []
    for expert in range(local_experts):
        rows = spread[:, :, expert].reshape(seq_ranks * shards * count, width)
        gate = jnp.dot(rows, w_gate[expert], preferred_element_type=jnp.float32)
        upper = jnp.dot(rows, w_up[expert], preferred_element_type=jnp.float32)
        hidden = (jax.nn.silu(gate) * upper).astype(jnp.bfloat16)
        part = jnp.dot(hidden, w_down[expert], preferred_element_type=jnp.float32).astype(
            jnp.bfloat16
        )
        partials.append(part.reshape(seq_ranks, shards, count, width))
    stacked = jnp.stack(partials, axis=2)
    summed = lax.psum_scatter(stacked, "tp", scatter_dimension=1, tiled=True).astype(jnp.float32)
    returned = lax.all_to_all(
        summed[:, 0].astype(jnp.bfloat16), "sp", split_axis=0, concat_axis=0, tiled=True
    )
    results = returned.reshape(experts * capacity, width)[slot]
    results = results.reshape(block_rows, 2, width).astype(jnp.float32)
    weighted = jnp.sum(route_weight[:, :, None] * results, axis=1)
    return (stream + weighted).astype(jnp.bfloat16)


def dot(a, b):
    return jnp.dot(a, b, preferred_element_type=F32)


ORDER = (
    "P00 F10 E00 P01",
    "F11 E01 A00 F20",
    "P10 E10 F21 P11",
    "E11 A10 A11 F30",
    "P20 E20 F31 P21",
    "E21 A20 A21 B10",
    "P30 E30 B11 P31",
    "E31 A30 A31 B20",
    "B21 A01 B30 B31",
    "B00 B01",
)


def fused_kernel(
    input_hbm,
    pre_hbm,
    post_hbm,
    taps_hbm,
    proj_hbm,
    residual_hbm,
    gain_hbm,
    routes_hbm,
    weight_hbm,
    gate_hbm,
    up_hbm,
    down_hbm,
    out,
    conv_input,
    pre_gate,
    post_gate,
    conv_taps,
    proj,
    residual,
    gain,
    routes,
    route_weight,
    w_gate,
    w_up,
    w_down,
    halo,
    gated,
    mix_out,
    mix_in,
    stream,
    weigh_out,
    weigh,
    leaving,
    tok,
    begun,
    hidden,
    part,
    from_core,
    kept,
    to_chip,
    from_chip,
    to_home,
    home,
    known,
    load_sem,
    sent,
    halo_recv,
    mix_recv,
    weigh_recv,
    z_recv,
    x_recv,
    core_recv,
    one_recv,
    two_recv,
    home_recv,
):
    s, t = lax.axis_index("sp"), lax.axis_index("tp")
    rows, width = residual.shape
    half = width // 2
    channels = conv_input.shape[1]
    cap = rows // GROUPS
    units = w_gate.shape[2]
    core, chip, far = t + 1 - 2 * (t % 2), (t + 2) % 4, 3 - t
    sp_of = [s, s + 1 - 2 * (s % 2), (s + 2) % 4, 3 - s]
    pos = lambda place: (place % 2) * 2 + place // 2
    middle = (s == 1) | (s == 2)
    X_SENT, Z_SENT, ONE_SENT, TWO_SENT, MIX_SENT, WEIGH_SENT, HALO_SENT = range(7)

    def describe(src, dst, group, recv_sem, **where):
        return pltpu.make_async_remote_copy(
            src_ref=src,
            dst_ref=dst,
            send_sem=sent.at[group],
            recv_sem=recv_sem,
            device_id=where,
            device_id_type=pl.DeviceIdType.MESH,
        )

    def send(*refs, **where):
        describe(*refs, **where).start()

    def wait_for(piece, sem):
        pltpu.make_async_copy(piece, piece, sem).wait()

    def signal(sem, **where):
        pl.semaphore_signal(sem, inc=1, device_id=where, device_id_type=pl.DeviceIdType.MESH)

    barrier = pltpu.get_barrier_semaphore()
    signal(barrier, sp=sp_of[1])

    @pl.when(middle)
    def _():
        signal(barrier, sp=sp_of[3])

    for other in (core, chip, far):
        signal(barrier, tp=other)
    loads = []
    for i, (a, b) in enumerate(
        (
            (input_hbm, conv_input),
            (pre_hbm, pre_gate),
            (post_hbm, post_gate),
            (taps_hbm, conv_taps),
            (routes_hbm, routes),
            (weight_hbm, route_weight),
            (gain_hbm, gain),
            (residual_hbm, residual),
            (proj_hbm, proj),
            (gate_hbm, w_gate),
            (up_hbm, w_up),
            (down_hbm, w_down),
        )
    ):
        loads.append(pltpu.make_async_copy(a, b, load_sem.at[i]))
    for load in loads[:7]:
        load.start()
    for load in loads[:4]:
        load.wait()
    for load in loads[7:]:
        load.start()

    count = conv_input.shape[0]
    gated[pl.ds(8, count), :] = pre_gate[...].astype(F32) * conv_input[...].astype(F32)
    taps = conv_taps[:, pl.ds(pl.multiple_of(t * channels, channels), channels)]

    def mix(place, low, size):
        start = pl.multiple_of(place * rows, rows) + low
        g = gated[pl.ds(start, size + 8), :]
        conv = g[8:] * taps[2:3] + g[7:-1] * taps[1:2] + g[6:-2] * taps[0:1]
        return (post_gate[pl.ds(start, size), :].astype(F32) * conv).astype(BF16)

    edge = 16
    partners = (chip, far, core)

    def send_mixed(i, low, size):
        piece = pl.ds(low, size)
        send(
            mix_out.at[i, piece, :],
            mix_in.at[t, piece, :],
            MIX_SENT,
            mix_recv.at[t],
            tp=partners[i],
        )

    def wait_mixed(place):
        wait_for(mix_in.at[place], mix_recv.at[place])

    gated[0:8, :] = jnp.zeros((8, channels), F32)
    for i in range(3):
        mix_out[i] = mix(partners[i], 0, rows)

    @pl.when(middle)
    def _():
        pl.semaphore_wait(barrier, 5)

    @pl.when(jnp.logical_not(middle))
    def _():
        pl.semaphore_wait(barrier, 4)

    def halo_copy(i):
        ref = (conv_input, pre_gate)[i]
        return describe(
            ref.at[pl.ds(count - 16, 16), :],
            halo.at[i],
            HALO_SENT,
            halo_recv.at[0],
            sp=(s + 1) % 4,
        )

    @pl.when(s < 3)
    def _():
        for i in range(2):
            halo_copy(i).start()

    for i in range(3):

        @pl.when(partners[i] > 0)
        def _():
            send_mixed(i, 0, rows)

        @pl.when(partners[i] == 0)
        def _():
            send_mixed(i, edge, rows - edge)

    @pl.when(middle)
    def _():
        signal(known, sp=sp_of[3])
        signal(known, sp=sp_of[1])

    for load in loads[4:6]:
        load.wait()
    first, second = routes[0:1, :], routes[1:2, :]
    epg = w_gate.shape[0]
    down = lax.broadcasted_iota(jnp.int32, (rows, rows), 0)
    across = lax.broadcasted_iota(jnp.int32, (rows, rows), 1)
    group = lax.broadcasted_iota(jnp.int32, (16, rows), 0)
    member = (first >= group * epg) & (first < group * epg + epg) & (group < GROUPS)
    member = jnp.where(member, 1.0, 0.0)
    earlier = jnp.where(down < across, 1.0, 0.0).astype(BF16)
    rank = dot(member.astype(BF16), earlier)
    slot = jnp.sum(member * (rank + (group * cap).astype(F32)), axis=0, keepdims=True)
    pick = jnp.where(slot == down.astype(F32), 1.0, 0.0)
    back = pick.T.astype(BF16)
    pick = pick.astype(BF16)
    low = jnp.where(first < second, route_weight[0:1, :], route_weight[1:2, :])
    high = jnp.where(first < second, route_weight[1:2, :], route_weight[0:1, :])
    low_top, high_top = low.astype(BF16).astype(F32), high.astype(BF16).astype(F32)
    line = lax.broadcasted_iota(jnp.int32, (LANES, rows), 0)
    scales = jnp.where(
        line == 0,
        low_top,
        jnp.where(
            line == 1,
            low - low_top,
            jnp.where(line == 2, high_top, jnp.where(line == 3, high - high_top, 0.0)),
        ),
    ).astype(BF16)
    scales = lax.dot_general(
        pick, scales, (((1,), (1,)), ((), ())), preferred_element_type=F32
    )
    weigh_out[...] = scales.astype(BF16)

    @pl.when(s > 0)
    def _():
        wait_for(halo, halo_recv.at[0])
        gated[0:8, :] = halo[0, 8:16, :].astype(F32) * halo[1, 8:16, :].astype(F32)

    for i in range(3):

        @pl.when(partners[i] == 0)
        def _():
            mix_out[i, 0:edge, :] = mix(0, 0, edge)
            send_mixed(i, 0, edge)

    mix_in[t] = mix(t, 0, rows)

    @pl.when(middle)
    def _():
        pl.semaphore_wait(known, 1)
        signal(known, sp=sp_of[1])

    @pl.when(jnp.logical_not(middle))
    def _():
        pl.semaphore_wait(known, 2)

    group_rows = lambda g: pl.ds(pl.multiple_of(g * cap, cap), cap)
    block = lambda place: pl.ds(pl.multiple_of(pos(place) * cap, cap), cap)
    for k in (1, 2, 3):
        send(
            weigh_out.at[group_rows(sp_of[k]), :],
            weigh.at[s, block(t), :],
            WEIGH_SENT,
            weigh_recv.at[0],
            sp=sp_of[k],
        )
    weigh[s, block(t), :] = weigh_out[group_rows(s), :]

    def forward_weigh():
        wait_for(weigh.at[0:3, 0:cap, :], weigh_recv.at[0])
        for k in range(4):
            mine = weigh.at[sp_of[k], block(t), :]
            src = mine if k else weigh_out.at[group_rows(s), :]
            send(src, mine, WEIGH_SENT, weigh_recv.at[1], tp=chip)
            send(src, mine, WEIGH_SENT, weigh_recv.at[2], tp=core)

    def pass_weigh():
        wait_for(weigh.at[:, 0:cap, :], weigh_recv.at[1])
        for k in range(4):
            arrived = weigh.at[sp_of[k], block(chip), :]
            send(arrived, arrived, WEIGH_SENT, weigh_recv.at[2], tp=core)

    tile = 512
    tiles = width // tile
    column = lambda n: pl.ds(pl.multiple_of(n * tile, tile), tile)
    weights_of = lambda place: pl.ds(pl.multiple_of(place * channels, channels), channels)
    loads[7].wait()
    loads[8].wait()
    wait_mixed(core)

    def project_near(n, carry):
        cols = column(n)
        total = residual[:, cols].astype(F32)
        for place in (t, core):
            total += dot(mix_in[place], proj[weights_of(place), cols])
        stream[:, cols] = total
        return carry

    lax.fori_loop(0, tiles, project_near, 0)
    wait_mixed(chip)

    def project_chip(n, carry):
        cols = column(n)
        stream[:, cols] += dot(mix_in[chip], proj[weights_of(chip), cols])
        return carry

    lax.fori_loop(0, tiles, project_chip, 0)
    forward_weigh()
    wait_mixed(far)

    def project_far(n, squares):
        cols = column(n)
        total = stream[:, cols] + dot(mix_in[far], proj[weights_of(far), cols])
        stream[:, cols] = total
        return squares + jnp.sum(total * total, axis=1, keepdims=True)

    squares = lax.fori_loop(0, tiles, project_far, jnp.zeros((rows, 1), F32))
    scale = lax.rsqrt(squares / width + 1e-06)
    loads[6].wait()

    def forward(k, h):
        dst = tok.at[sp_of[k], h, block(t), :]
        src = leaving.at[h, group_rows(s), :]
        if k:
            wait_for(dst, z_recv.at[2 * k + h - 2])
            src = dst
        i = 2 * k + h
        send(src, dst, X_SENT, x_recv.at[i], tp=chip)
        send(src, dst, X_SENT, core_recv.at[i], tp=core)
        if not k:
            tok[s, h, block(t), :] = leaving[h, group_rows(s), :]

    def leave(k, h):
        send(
            leaving.at[h, group_rows(sp_of[k]), :],
            tok.at[s, h, block(t), :],
            Z_SENT,
            z_recv.at[2 * k + h - 2],
            sp=sp_of[k],
        )

    for h in (0, 1):

        def norm(n, carry):
            cols = column(n + h * (tiles // 2))
            row = (stream[:, cols] * scale * gain[:, cols]).astype(BF16)
            leaving[h, :, column(n)] = dot(pick, row).astype(BF16)
            return carry

        lax.fori_loop(0, tiles // 2, norm, 0)
        if h == 0:
            leave(1, 0)
            forward(0, 0)
    for k, h in ((1, 1), (2, 0), (2, 1), (3, 0), (3, 1)):
        leave(k, h)
    forward(0, 1)
    pass_weigh()
    for load in loads[9:]:
        load.wait()

    def pass_on(k, h):
        i = 2 * k + h
        arrived = tok.at[sp_of[k], h, block(chip), :]
        wait_for(arrived, x_recv.at[i])
        send(arrived, arrived, X_SENT, core_recv.at[i], tp=core)

    weighed = []
    core_rows = lambda c: pl.ds(pl.multiple_of(c * 2 * cap, cap), 2 * cap)

    def experts(k, h):
        g = sp_of[k]
        wait_for(tok.at[g, h, 0 : 2 * cap, :], core_recv.at[2 * k + h])
        x = tok[g, h]
        deep = pl.ds(h * half, half)
        if h == 0:
            for e in range(epg):
                begun[2 * e] = dot(x, w_gate[e, deep, :])
                begun[2 * e + 1] = dot(x, w_up[e, deep, :])
            return
        if not weighed:
            wait_for(weigh.at[:, 0 : 2 * cap, :], weigh_recv.at[2])
            weighed.append(True)
        top = weigh[g].astype(F32)
        for e in range(epg):
            w = top[:, 2 * e : 2 * e + 1] + top[:, 2 * e + 1 : 2 * e + 2]
            gate = begun[2 * e] + dot(x, w_gate[e, deep, :])
            upper = begun[2 * e + 1] + dot(x, w_up[e, deep, :])
            act = gate / (1.0 + jnp.exp(-gate)) * upper * w
            hidden[:, pl.ds(e * units, units)] = act.astype(BF16)
        for h in (0, 1):

            def lower(n, carry):
                cols = column(n + h * (tiles // 2))
                part[k, h, :, column(n)] = dot(hidden[...], w_down[:, cols]).astype(BF16)
                return carry

            lax.fori_loop(0, tiles // 2, lower, 0)
            i = 2 * k + h
            send(
                part.at[k, h, core_rows(1 - t % 2), :],
                from_core.at[k, h],
                ONE_SENT,
                one_recv.at[i],
                tp=core,
            )

    def add_core(k, h):
        i = 2 * k + h
        wait_for(from_core.at[k, h], one_recv.at[i])
        for mine in (False, True):
            x = t // 2 if mine else 1 - t // 2
            base = pl.multiple_of((t % 2) * 2 * cap + x * cap, cap)
            near = pl.multiple_of(x * cap, cap)
            total = part[k, h, pl.ds(base, cap), :].astype(F32)
            total += from_core[k, h, pl.ds(near, cap), :].astype(F32)
            if mine:
                kept[k, h] = total
            else:
                to_chip[k, h] = total.astype(BF16)
                send(
                    to_chip.at[k, h],
                    from_chip.at[k, h],
                    TWO_SENT,
                    two_recv.at[i],
                    tp=chip,
                )

    def add_chip(k, h):
        wait_for(from_chip.at[k, h], two_recv.at[2 * k + h])
        total = (kept[k, h] + from_chip[k, h].astype(F32)).astype(BF16)
        if k == 0:
            home[h, group_rows(s), :] = total
        else:
            to_home[k, h] = total
            send(
                to_home.at[k, h],
                home.at[h, group_rows(s), :],
                Z_SENT,
                home_recv.at[h],
                sp=sp_of[k],
            )

    stages = dict(F=forward, P=pass_on, E=experts, A=add_core, B=add_chip)
    for line_of in ORDER:
        for stage in line_of.split():
            stages[stage[0]](*map(int, stage[1:]))

    for h in (0, 1):

        def finish(n, carry):
            cols = column(n + h * (tiles // 2))
            out[:, cols] = (stream[:, cols] + dot(back, home[h, :, column(n)])).astype(BF16)
            return carry

        wait_for(home.at[h, 0 : 3 * cap, :], home_recv.at[h])
        lax.fori_loop(0, tiles // 2, finish, 0)
    wait_for(tok.at[0:3], sent.at[X_SENT])
    wait_for(tok.at[0:3, :, 0 : 2 * cap, :], sent.at[Z_SENT])
    wait_for(tok.at[0:2], sent.at[ONE_SENT])
    wait_for(tok.at[0], sent.at[TWO_SENT])
    wait_for(mix_out, sent.at[MIX_SENT])
    wait_for(weigh.at[0:3], sent.at[WEIGH_SENT])
    wait_for(weigh.at[0:3, 0:cap, :], sent.at[WEIGH_SENT])

    @pl.when(s < 3)
    def _():
        wait_for(halo, sent.at[HALO_SENT])


def fused(*args):
    (conv_input, _, _, _, out_proj, residual, gain, _, _, w_gate, w_up, w_down) = args
    rows, width = residual.shape
    count, channels = conv_input.shape
    local, _, units = w_gate.shape
    cap = rows // GROUPS
    half = width // 2
    w_down = w_down.reshape(local * units, width)
    args = args[:6] + (gain.reshape(1, width), args[7].T, args[8].T) + args[9:11] + (w_down,)
    far = pl.BlockSpec(memory_space=pl.ANY)
    vmem, sems = pltpu.VMEM, pltpu.SemaphoreType.DMA
    return pl.pallas_call(
        fused_kernel,
        out_shape=vmem((rows, width), BF16),
        in_specs=[far] * 12,
        out_specs=pl.BlockSpec(memory_space=vmem),
        scratch_shapes=[vmem(arg.shape, arg.dtype) for arg in args]
        + [
            vmem((2, 16, channels), BF16),
            vmem((count + 8, channels), F32),
            vmem((3, rows, channels), BF16),
            vmem((4, rows, channels), BF16),
            vmem((rows, width), F32),
            vmem((rows, LANES), BF16),
            vmem((4, rows, LANES), BF16),
            vmem((2, rows, half), BF16),
            vmem((4, 2, rows, half), BF16),
            vmem((2 * local, rows, units), F32),
            vmem((rows, local * units), BF16),
            vmem((4, 2, rows, half), BF16),
            vmem((4, 2, 2 * cap, half), BF16),
            vmem((4, 2, cap, half), F32),
            vmem((4, 2, cap, half), BF16),
            vmem((4, 2, cap, half), BF16),
            vmem((4, 2, cap, half), BF16),
            vmem((2, rows, half), BF16),
            pltpu.SemaphoreType.REGULAR,
        ]
        + [sems((n,)) for n in (12, 7, 1, 4, 3, 6, 8, 8, 8, 8, 2)],
        compiler_params=pltpu.CompilerParams(
            collective_id=0, has_side_effects=True, vmem_limit_bytes=56 << 20
        ),
    )(*args)


def on_device(*args):
    residual, routes, w_gate = args[5], args[7], args[9]
    rows, local, seq_ranks = residual.shape[0], w_gate.shape[0], lax.axis_size("sp")
    dense = local == routes.shape[1] == 2 and local * seq_ranks == local * GROUPS
    if dense and lax.axis_size("tp") == 4 and rows % LANES == 0:
        return fused(*args)
    return generic(*args)


def solution(mesh):
    return jax.shard_map(
        on_device,
        mesh=mesh,
        in_specs=(
            P(("grp", "sp"), "tp"),
            P(("grp", "sp"), "tp"),
            P(("grp", "sp"), "tp"),
            P(),
            P(),
            P(("grp", "sp", "tp"), None),
            P(),
            P(("grp", "sp", "tp"), None),
            P(("grp", "sp", "tp"), None),
            P("sp", None, "tp"),
            P("sp", None, "tp"),
            P("sp", "tp", None),
        ),
        out_specs=P(("grp", "sp", "tp"), None),
        check_vma=False,
    )
```

```python
import functools

import jax
import jax.numpy as jnp
from jax import lax
from jax.experimental import pallas as pl
from jax.experimental.pallas import tpu as pltpu
from jax.sharding import PartitionSpec as P

GROUPS = 4
LANES = 128
F32, BF16 = jnp.float32, jnp.bfloat16


def shifted(block, axis, distance):
    devices = range(lax.axis_size(axis))
    route = [(i - distance, i) for i in devices if i - distance in devices]
    return lax.ppermute(block, axis, route)


def generic(
    conv_input,
    pre_gate,
    post_gate,
    conv_taps,
    out_proj,
    residual_in,
    norm_gain,
    routes,
    route_weight,
    w_gate,
    w_up,
    w_down,
):
    shards = lax.axis_size("tp")
    place = lax.axis_index("tp")
    seq_ranks = lax.axis_size("sp")
    channels = conv_input.shape[1]
    width = residual_in.shape[1]
    taps = lax.dynamic_slice_in_dim(conv_taps, place * channels, channels, 1)
    prior_input, prior_gate = shifted((conv_input[-2:], pre_gate[-2:]), "sp", 1)
    gated = jnp.concatenate(
        [
            prior_gate.astype(jnp.float32) * prior_input.astype(jnp.float32),
            pre_gate.astype(jnp.float32) * conv_input.astype(jnp.float32),
        ],
        axis=0,
    )
    conv = gated[2:] * taps[2] + gated[1:-1] * taps[1] + gated[:-2] * taps[0]
    mixed = (post_gate.astype(jnp.float32) * conv).astype(jnp.bfloat16)
    token_rows = lax.all_to_all(mixed, "tp", split_axis=0, concat_axis=1, tiled=True)
    projected = jnp.dot(token_rows, out_proj, preferred_element_type=jnp.float32)
    stream = residual_in.astype(jnp.float32) + projected
    scale = lax.rsqrt(jnp.mean(stream * stream, axis=-1, keepdims=True) + 1e-06)
    normed = (stream * scale * norm_gain).astype(jnp.bfloat16)
    block_rows = routes.shape[0]
    local_experts = w_gate.shape[0]
    experts = local_experts * seq_ranks
    capacity = 2 * block_rows // experts
    flat_routes = routes.reshape(-1)
    position = jnp.arange(flat_routes.shape[0], dtype=jnp.int32)
    earlier = (flat_routes[:, None] == flat_routes[None, :]) & (
        position[None, :] < position[:, None]
    )
    rank = jnp.sum(earlier.astype(jnp.int32), axis=1)
    slot = flat_routes * capacity + rank
    outgoing = (
        jnp.zeros((experts * capacity, width), jnp.bfloat16).at[slot].set(normed[position // 2])
    )
    outgoing = outgoing.reshape(seq_ranks, local_experts, capacity, width)
    spread = lax.all_gather(
        lax.all_to_all(outgoing, "sp", split_axis=0, concat_axis=0, tiled=True)[:, None],
        "tp",
        axis=1,
        tiled=True,
    )
    count = spread.shape[3]
    partials = []
    for expert in range(local_experts):
        rows = spread[:, :, expert].reshape(seq_ranks * shards * count, width)
        gate = jnp.dot(rows, w_gate[expert], preferred_element_type=jnp.float32)
        upper = jnp.dot(rows, w_up[expert], preferred_element_type=jnp.float32)
        hidden = (jax.nn.silu(gate) * upper).astype(jnp.bfloat16)
        part = jnp.dot(hidden, w_down[expert], preferred_element_type=jnp.float32).astype(
            jnp.bfloat16
        )
        partials.append(part.reshape(seq_ranks, shards, count, width))
    stacked = jnp.stack(partials, axis=2)
    summed = lax.psum_scatter(stacked, "tp", scatter_dimension=1, tiled=True).astype(jnp.float32)
    returned = lax.all_to_all(
        summed[:, 0].astype(jnp.bfloat16), "sp", split_axis=0, concat_axis=0, tiled=True
    )
    results = returned.reshape(experts * capacity, width)[slot]
    results = results.reshape(block_rows, 2, width).astype(jnp.float32)
    weighted = jnp.sum(route_weight[:, :, None] * results, axis=1)
    return (stream + weighted).astype(jnp.bfloat16)


def dot(a, b):
    return jnp.dot(a, b, preferred_element_type=F32)


EARLY = ("Z10 F00",)
ORDER = (
    "Z11 Z20 Z21 Z30",
    "Z31 F01 W P00",
    "F10 E00 V P01",
    "F11 Y E01 L00",
    "L01 A00 F20 P10",
    "E10 F21 P11 E11",
    "L10 L11 A10 A11",
    "F30 P20 F31 P21",
    "E20 E21 L20 L21",
    "A20 A21 B10 P30",
    "E30 A01 B11 P31",
    "E31 L30 L31 A30",
    "B20 B21 A31 B30",
    "B00 B01 B31",
)
ORDERS = (ORDER, ORDER, ORDER, ORDER)


def fused_kernel(
    input_hbm,
    pre_hbm,
    post_hbm,
    taps_hbm,
    proj_hbm,
    residual_hbm,
    gain_hbm,
    routes_hbm,
    weight_hbm,
    gate_hbm,
    up_hbm,
    down_hbm,
    out,
    conv_input,
    pre_gate,
    post_gate,
    conv_taps,
    proj,
    residual,
    gain,
    routes,
    route_weight,
    w_gate,
    w_up,
    w_down,
    halo,
    gated,
    mix_out,
    mix_in,
    stream,
    weigh_out,
    weigh,
    leaving,
    tok,
    begun,
    hidden,
    part,
    from_core,
    kept,
    to_chip,
    from_chip,
    to_home,
    home,
    known,
    load_sem,
    sent,
    halo_recv,
    mix_recv,
    weigh_recv,
    z_recv,
    x_recv,
    core_recv,
    one_recv,
    two_recv,
    home_recv,
):
    s, t = lax.axis_index("sp"), lax.axis_index("tp")
    rows, width = residual.shape
    half = width // 2
    channels = conv_input.shape[1]
    cap = rows // GROUPS
    units = w_gate.shape[2]
    core, chip, far = t + 1 - 2 * (t % 2), (t + 2) % 4, 3 - t
    sp_of = [s, s + 1 - 2 * (s % 2), (s + 2) % 4, 3 - s]
    pos = lambda place: (place % 2) * 2 + place // 2
    middle = (s == 1) | (s == 2)
    X_SENT, Z_SENT, ONE_SENT, TWO_SENT, MIX_SENT, WEIGH_SENT, HALO_SENT = range(7)

    def describe(src, dst, group, recv_sem, **where):
        return pltpu.make_async_remote_copy(
            src_ref=src,
            dst_ref=dst,
            send_sem=sent.at[group],
            recv_sem=recv_sem,
            device_id=where,
            device_id_type=pl.DeviceIdType.MESH,
        )

    def send(*refs, **where):
        describe(*refs, **where).start()

    def wait_for(piece, sem):
        pltpu.make_async_copy(piece, piece, sem).wait()

    def signal(sem, **where):
        pl.semaphore_signal(sem, inc=1, device_id=where, device_id_type=pl.DeviceIdType.MESH)

    barrier = pltpu.get_barrier_semaphore()
    signal(barrier, sp=sp_of[1])

    @pl.when(middle)
    def _():
        signal(barrier, sp=sp_of[3])

    for other in (core, chip, far):
        signal(barrier, tp=other)
    loads = []
    for i, (a, b) in enumerate(
        (
            (input_hbm, conv_input),
            (pre_hbm, pre_gate),
            (post_hbm, post_gate),
            (taps_hbm, conv_taps),
            (routes_hbm, routes),
            (weight_hbm, route_weight),
            (gain_hbm, gain),
            (residual_hbm, residual),
            (proj_hbm, proj),
            (gate_hbm, w_gate),
            (up_hbm, w_up),
            (down_hbm, w_down),
        )
    ):
        loads.append(pltpu.make_async_copy(a, b, load_sem.at[i]))
    for load in loads[:7]:
        load.start()
    for load in loads[:4]:
        load.wait()
    for load in loads[7:]:
        load.start()

    count = conv_input.shape[0]
    gated[pl.ds(8, count), :] = pre_gate[...].astype(F32) * conv_input[...].astype(F32)
    taps = conv_taps[:, pl.ds(pl.multiple_of(t * channels, channels), channels)]

    def mix(place, low, size):
        start = pl.multiple_of(place * rows, rows) + low
        g = gated[pl.ds(start, size + 8), :]
        conv = g[8:] * taps[2:3] + g[7:-1] * taps[1:2] + g[6:-2] * taps[0:1]
        return (post_gate[pl.ds(start, size), :].astype(F32) * conv).astype(BF16)

    edge = 16
    partners = (chip, far, core)

    def send_mixed(i, low, size):
        piece = pl.ds(low, size)
        send(
            mix_out.at[i, piece, :],
            mix_in.at[t, piece, :],
            MIX_SENT,
            mix_recv.at[t],
            tp=partners[i],
        )

    def wait_mixed(place):
        wait_for(mix_in.at[place], mix_recv.at[place])

    gated[0:8, :] = jnp.zeros((8, channels), F32)
    for i in range(3):
        mix_out[i] = mix(partners[i], 0, rows)

    @pl.when(middle)
    def _():
        pl.semaphore_wait(barrier, 5)

    @pl.when(jnp.logical_not(middle))
    def _():
        pl.semaphore_wait(barrier, 4)

    def halo_copy(i):
        ref = (conv_input, pre_gate)[i]
        return describe(
            ref.at[pl.ds(count - 16, 16), :],
            halo.at[i],
            HALO_SENT,
            halo_recv.at[0],
            sp=(s + 1) % 4,
        )

    @pl.when(s < 3)
    def _():
        for i in range(2):
            halo_copy(i).start()

    for i in range(3):

        @pl.when(partners[i] > 0)
        def _():
            send_mixed(i, 0, rows)

        @pl.when(partners[i] == 0)
        def _():
            send_mixed(i, edge, rows - edge)

    @pl.when(middle)
    def _():
        signal(known, sp=sp_of[3])
        signal(known, sp=sp_of[1])

    for load in loads[4:6]:
        load.wait()
    first, second = routes[0:1, :], routes[1:2, :]
    epg = w_gate.shape[0]
    down = lax.broadcasted_iota(jnp.int32, (rows, rows), 0)
    across = lax.broadcasted_iota(jnp.int32, (rows, rows), 1)
    group = lax.broadcasted_iota(jnp.int32, (16, rows), 0)
    member = (first >= group * epg) & (first < group * epg + epg) & (group < GROUPS)
    member = jnp.where(member, 1.0, 0.0)
    earlier = jnp.where(down < across, 1.0, 0.0).astype(BF16)
    rank = dot(member.astype(BF16), earlier)
    slot = jnp.sum(member * (rank + (group * cap).astype(F32)), axis=0, keepdims=True)
    pick = jnp.where(slot == down.astype(F32), 1.0, 0.0)
    back = pick.T.astype(BF16)
    pick = pick.astype(BF16)
    low = jnp.where(first < second, route_weight[0:1, :], route_weight[1:2, :])
    high = jnp.where(first < second, route_weight[1:2, :], route_weight[0:1, :])
    low_top, high_top = low.astype(BF16).astype(F32), high.astype(BF16).astype(F32)
    line = lax.broadcasted_iota(jnp.int32, (LANES, rows), 0)
    scales = jnp.where(
        line == 0,
        low_top,
        jnp.where(
            line == 1,
            low - low_top,
            jnp.where(line == 2, high_top, jnp.where(line == 3, high - high_top, 0.0)),
        ),
    ).astype(BF16)
    scales = lax.dot_general(
        pick, scales, (((1,), (1,)), ((), ())), preferred_element_type=F32
    )
    weigh_out[...] = scales.astype(BF16)

    @pl.when(s > 0)
    def _():
        wait_for(halo, halo_recv.at[0])
        gated[0:8, :] = halo[0, 8:16, :].astype(F32) * halo[1, 8:16, :].astype(F32)

    for i in range(3):

        @pl.when(partners[i] == 0)
        def _():
            mix_out[i, 0:edge, :] = mix(0, 0, edge)
            send_mixed(i, 0, edge)

    mix_in[t] = mix(t, 0, rows)

    @pl.when(middle)
    def _():
        pl.semaphore_wait(known, 1)
        signal(known, sp=sp_of[1])

    group_rows = lambda g: pl.ds(pl.multiple_of(g * cap, cap), cap)
    block = lambda place: pl.ds(pl.multiple_of(pos(place) * cap, cap), cap)
    weigh[s, block(t), :] = weigh_out[group_rows(s), :]

    def forward_weigh():
        wait_for(weigh.at[0:3, 0:cap, :], weigh_recv.at[0])
        for k in range(4):
            mine = weigh.at[sp_of[k], block(t), :]
            src = mine if k else weigh_out.at[group_rows(s), :]
            send(src, mine, WEIGH_SENT, weigh_recv.at[1], tp=chip)
            send(src, mine, WEIGH_SENT, weigh_recv.at[2], tp=core)

    def pass_weigh():
        wait_for(weigh.at[:, 0:cap, :], weigh_recv.at[1])
        for k in range(4):
            arrived = weigh.at[sp_of[k], block(chip), :]
            send(arrived, arrived, WEIGH_SENT, weigh_recv.at[2], tp=core)

    tile = 512
    tiles = width // tile
    column = lambda n: pl.ds(pl.multiple_of(n * tile, tile), tile)
    weights_of = lambda place: pl.ds(pl.multiple_of(place * channels, channels), channels)
    loads[7].wait()
    loads[8].wait()
    wait_mixed(core)

    def project_near(n, carry):
        cols = column(n)
        total = residual[:, cols].astype(F32)
        for place in (t, core):
            total += dot(mix_in[place], proj[weights_of(place), cols])
        stream[:, cols] = total
        return carry

    lax.fori_loop(0, tiles, project_near, 0)
    wait_mixed(chip)

    def project_chip(n, carry):
        cols = column(n)
        stream[:, cols] += dot(mix_in[chip], proj[weights_of(chip), cols])
        return carry

    lax.fori_loop(0, tiles, project_chip, 0)

    @pl.when(jnp.logical_not(middle))
    def _():
        pl.semaphore_wait(known, 2)

    for k in (1, 2, 3):
        send(
            weigh_out.at[group_rows(sp_of[k]), :],
            weigh.at[s, block(t), :],
            WEIGH_SENT,
            weigh_recv.at[0],
            sp=sp_of[k],
        )
    wait_mixed(far)

    def project_far(n, squares):
        cols = column(n)
        total = stream[:, cols] + dot(mix_in[far], proj[weights_of(far), cols])
        stream[:, cols] = total
        return squares + jnp.sum(total * total, axis=1, keepdims=True)

    squares = lax.fori_loop(0, tiles, project_far, jnp.zeros((rows, 1), F32))
    scale = lax.rsqrt(squares / width + 1e-06)
    loads[6].wait()

    def forward(k, h):
        dst = tok.at[sp_of[k], h, block(t), :]
        src = leaving.at[h, group_rows(s), :]
        if k:
            wait_for(dst, z_recv.at[2 * k + h - 2])
            src = dst
        i = 2 * k + h
        send(src, dst, X_SENT, x_recv.at[i], tp=chip)
        send(src, dst, X_SENT, core_recv.at[i], tp=core)
        if not k:
            tok[s, h, block(t), :] = leaving[h, group_rows(s), :]

    def leave(k, h):
        send(
            leaving.at[h, group_rows(sp_of[k]), :],
            tok.at[s, h, block(t), :],
            Z_SENT,
            z_recv.at[2 * k + h - 2],
            sp=sp_of[k],
        )

    for h in (0, 1):

        def norm(n, carry):
            cols = column(n + h * (tiles // 2))
            row = (stream[:, cols] * scale * gain[:, cols]).astype(BF16)
            leaving[h, :, column(n)] = dot(pick, row).astype(BF16)
            return carry

        lax.fori_loop(0, tiles // 2, norm, 0)
        if h == 0:
            for stage in " ".join(EARLY).split():
                (leave if stage[0] == "Z" else forward)(*map(int, stage[1:]))

    for load in loads[9:]:
        load.wait()

    def pass_on(k, h):
        i = 2 * k + h
        arrived = tok.at[sp_of[k], h, block(chip), :]
        wait_for(arrived, x_recv.at[i])
        send(arrived, arrived, X_SENT, core_recv.at[i], tp=core)

    core_rows = lambda c: pl.ds(pl.multiple_of(c * 2 * cap, cap), 2 * cap)

    def experts(k, h):
        g = sp_of[k]
        wait_for(tok.at[g, h, 0 : 2 * cap, :], core_recv.at[2 * k + h])
        x = tok[g, h]
        deep = pl.ds(h * half, half)
        if h == 0:
            for e in range(epg):
                begun[k, 2 * e] = dot(x, w_gate[e, deep, :])
                begun[k, 2 * e + 1] = dot(x, w_up[e, deep, :])
            return
        top = weigh[g].astype(F32)
        for e in range(epg):
            w = top[:, 2 * e : 2 * e + 1] + top[:, 2 * e + 1 : 2 * e + 2]
            gate = begun[k, 2 * e] + dot(x, w_gate[e, deep, :])
            upper = begun[k, 2 * e + 1] + dot(x, w_up[e, deep, :])
            act = gate / (1.0 + jnp.exp(-gate)) * upper * w
            hidden[k, :, pl.ds(e * units, units)] = act.astype(BF16)

    def lower(k, h):
        def step(n, carry):
            cols = column(n + h * (tiles // 2))
            part[k, h, :, column(n)] = dot(hidden[k], w_down[:, cols]).astype(BF16)
            return carry

        lax.fori_loop(0, tiles // 2, step, 0)
        send(
            part.at[k, h, core_rows(1 - t % 2), :],
            from_core.at[k, h],
            ONE_SENT,
            one_recv.at[2 * k + h],
            tp=core,
        )

    def add_core(k, h):
        i = 2 * k + h
        wait_for(from_core.at[k, h], one_recv.at[i])
        for mine in (False, True):
            x = t // 2 if mine else 1 - t // 2
            base = pl.multiple_of((t % 2) * 2 * cap + x * cap, cap)
            near = pl.multiple_of(x * cap, cap)
            total = part[k, h, pl.ds(base, cap), :].astype(F32)
            total += from_core[k, h, pl.ds(near, cap), :].astype(F32)
            if mine:
                kept[k, h] = total
            else:
                to_chip[k, h] = total.astype(BF16)
                send(
                    to_chip.at[k, h],
                    from_chip.at[k, h],
                    TWO_SENT,
                    two_recv.at[i],
                    tp=chip,
                )

    def add_chip(k, h):
        wait_for(from_chip.at[k, h], two_recv.at[2 * k + h])
        total = (kept[k, h] + from_chip[k, h].astype(F32)).astype(BF16)
        if k == 0:
            home[h, group_rows(s), :] = total
        else:
            to_home[k, h] = total
            send(
                to_home.at[k, h],
                home.at[h, group_rows(s), :],
                Z_SENT,
                home_recv.at[h],
                sp=sp_of[k],
            )

    stages = dict(
        F=forward,
        P=pass_on,
        E=experts,
        L=lower,
        A=add_core,
        B=add_chip,
        W=forward_weigh,
        V=pass_weigh,
        Y=lambda: wait_for(weigh.at[:, 0 : 2 * cap, :], weigh_recv.at[2]),
        Z=leave,
    )
    for order in dict.fromkeys(ORDERS):
        where = [i for i in range(4) if ORDERS[i] == order]

        def run():
            for stage in " ".join(order).split():
                stages[stage[0]](*map(int, stage[1:]))

        if len(where) == 4:
            run()
        else:
            chosen = functools.reduce(jnp.logical_or, [s == i for i in where])
            pl.when(chosen)(run)

    for h in (0, 1):

        def finish(n, carry):
            cols = column(n + h * (tiles // 2))
            out[:, cols] = (stream[:, cols] + dot(back, home[h, :, column(n)])).astype(BF16)
            return carry

        wait_for(home.at[h, 0 : 3 * cap, :], home_recv.at[h])
        lax.fori_loop(0, tiles // 2, finish, 0)
    wait_for(tok.at[0:3], sent.at[X_SENT])
    wait_for(tok.at[0:3, :, 0 : 2 * cap, :], sent.at[Z_SENT])
    wait_for(tok.at[0:2], sent.at[ONE_SENT])
    wait_for(tok.at[0], sent.at[TWO_SENT])
    wait_for(mix_out, sent.at[MIX_SENT])
    wait_for(weigh.at[0:3], sent.at[WEIGH_SENT])
    wait_for(weigh.at[0:3, 0:cap, :], sent.at[WEIGH_SENT])

    @pl.when(s < 3)
    def _():
        wait_for(halo, sent.at[HALO_SENT])


def fused(*args):
    (conv_input, _, _, _, out_proj, residual, gain, _, _, w_gate, w_up, w_down) = args
    rows, width = residual.shape
    count, channels = conv_input.shape
    local, _, units = w_gate.shape
    cap = rows // GROUPS
    half = width // 2
    w_down = w_down.reshape(local * units, width)
    args = args[:6] + (gain.reshape(1, width), args[7].T, args[8].T) + args[9:11] + (w_down,)
    far = pl.BlockSpec(memory_space=pl.ANY)
    vmem, sems = pltpu.VMEM, pltpu.SemaphoreType.DMA
    return pl.pallas_call(
        fused_kernel,
        out_shape=vmem((rows, width), BF16),
        in_specs=[far] * 12,
        out_specs=pl.BlockSpec(memory_space=vmem),
        scratch_shapes=[vmem(arg.shape, arg.dtype) for arg in args]
        + [
            vmem((2, 16, channels), BF16),
            vmem((count + 8, channels), F32),
            vmem((3, rows, channels), BF16),
            vmem((4, rows, channels), BF16),
            vmem((rows, width), F32),
            vmem((rows, LANES), BF16),
            vmem((4, rows, LANES), BF16),
            vmem((2, rows, half), BF16),
            vmem((4, 2, rows, half), BF16),
            vmem((4, 2 * local, rows, units), F32),
            vmem((4, rows, local * units), BF16),
            vmem((4, 2, rows, half), BF16),
            vmem((4, 2, 2 * cap, half), BF16),
            vmem((4, 2, cap, half), F32),
            vmem((4, 2, cap, half), BF16),
            vmem((4, 2, cap, half), BF16),
            vmem((4, 2, cap, half), BF16),
            vmem((2, rows, half), BF16),
            pltpu.SemaphoreType.REGULAR,
        ]
        + [sems((n,)) for n in (12, 7, 1, 4, 3, 6, 8, 8, 8, 8, 2)],
        compiler_params=pltpu.CompilerParams(
            collective_id=0, has_side_effects=True, vmem_limit_bytes=56 << 20
        ),
    )(*args)


def on_device(*args):
    residual, routes, w_gate = args[5], args[7], args[9]
    rows, local, seq_ranks = residual.shape[0], w_gate.shape[0], lax.axis_size("sp")
    dense = local == routes.shape[1] == 2 and local * seq_ranks == local * GROUPS
    if dense and lax.axis_size("tp") == 4 and rows % LANES == 0:
        return fused(*args)
    return generic(*args)


def solution(mesh):
    return jax.shard_map(
        on_device,
        mesh=mesh,
        in_specs=(
            P(("grp", "sp"), "tp"),
            P(("grp", "sp"), "tp"),
            P(("grp", "sp"), "tp"),
            P(),
            P(),
            P(("grp", "sp", "tp"), None),
            P(),
            P(("grp", "sp", "tp"), None),
            P(("grp", "sp", "tp"), None),
            P("sp", None, "tp"),
            P("sp", None, "tp"),
            P("sp", "tp", None),
        ),
        out_specs=P(("grp", "sp", "tp"), None),
        check_vma=False,
    )
```

```python
import functools

import jax
import jax.numpy as jnp
from jax import lax
from jax.experimental import pallas as pl
from jax.experimental.pallas import tpu as pltpu
from jax.sharding import PartitionSpec as P

GROUPS = 4
LANES = 128
F32, BF16 = jnp.float32, jnp.bfloat16


def shifted(block, axis, distance):
    devices = range(lax.axis_size(axis))
    route = [(i - distance, i) for i in devices if i - distance in devices]
    return lax.ppermute(block, axis, route)


def generic(
    conv_input,
    pre_gate,
    post_gate,
    conv_taps,
    out_proj,
    residual_in,
    norm_gain,
    routes,
    route_weight,
    w_gate,
    w_up,
    w_down,
):
    shards = lax.axis_size("tp")
    place = lax.axis_index("tp")
    seq_ranks = lax.axis_size("sp")
    channels = conv_input.shape[1]
    width = residual_in.shape[1]
    taps = lax.dynamic_slice_in_dim(conv_taps, place * channels, channels, 1)
    prior_input, prior_gate = shifted((conv_input[-2:], pre_gate[-2:]), "sp", 1)
    gated = jnp.concatenate(
        [
            prior_gate.astype(jnp.float32) * prior_input.astype(jnp.float32),
            pre_gate.astype(jnp.float32) * conv_input.astype(jnp.float32),
        ],
        axis=0,
    )
    conv = gated[2:] * taps[2] + gated[1:-1] * taps[1] + gated[:-2] * taps[0]
    mixed = (post_gate.astype(jnp.float32) * conv).astype(jnp.bfloat16)
    token_rows = lax.all_to_all(mixed, "tp", split_axis=0, concat_axis=1, tiled=True)
    projected = jnp.dot(token_rows, out_proj, preferred_element_type=jnp.float32)
    stream = residual_in.astype(jnp.float32) + projected
    scale = lax.rsqrt(jnp.mean(stream * stream, axis=-1, keepdims=True) + 1e-06)
    normed = (stream * scale * norm_gain).astype(jnp.bfloat16)
    block_rows = routes.shape[0]
    local_experts = w_gate.shape[0]
    experts = local_experts * seq_ranks
    capacity = 2 * block_rows // experts
    flat_routes = routes.reshape(-1)
    position = jnp.arange(flat_routes.shape[0], dtype=jnp.int32)
    earlier = (flat_routes[:, None] == flat_routes[None, :]) & (
        position[None, :] < position[:, None]
    )
    rank = jnp.sum(earlier.astype(jnp.int32), axis=1)
    slot = flat_routes * capacity + rank
    outgoing = (
        jnp.zeros((experts * capacity, width), jnp.bfloat16).at[slot].set(normed[position // 2])
    )
    outgoing = outgoing.reshape(seq_ranks, local_experts, capacity, width)
    spread = lax.all_gather(
        lax.all_to_all(outgoing, "sp", split_axis=0, concat_axis=0, tiled=True)[:, None],
        "tp",
        axis=1,
        tiled=True,
    )
    count = spread.shape[3]
    partials = []
    for expert in range(local_experts):
        rows = spread[:, :, expert].reshape(seq_ranks * shards * count, width)
        gate = jnp.dot(rows, w_gate[expert], preferred_element_type=jnp.float32)
        upper = jnp.dot(rows, w_up[expert], preferred_element_type=jnp.float32)
        hidden = (jax.nn.silu(gate) * upper).astype(jnp.bfloat16)
        part = jnp.dot(hidden, w_down[expert], preferred_element_type=jnp.float32).astype(
            jnp.bfloat16
        )
        partials.append(part.reshape(seq_ranks, shards, count, width))
    stacked = jnp.stack(partials, axis=2)
    summed = lax.psum_scatter(stacked, "tp", scatter_dimension=1, tiled=True).astype(jnp.float32)
    returned = lax.all_to_all(
        summed[:, 0].astype(jnp.bfloat16), "sp", split_axis=0, concat_axis=0, tiled=True
    )
    results = returned.reshape(experts * capacity, width)[slot]
    results = results.reshape(block_rows, 2, width).astype(jnp.float32)
    weighted = jnp.sum(route_weight[:, :, None] * results, axis=1)
    return (stream + weighted).astype(jnp.bfloat16)


def dot(a, b):
    return jnp.dot(a, b, preferred_element_type=F32)


EARLY = ("Z10 F00",)
ORDER = (
    "Z11 Z20 Z21 Z30",
    "Z31 F01 W P00",
    "F10 E00 V P01",
    "F11 Y E01 L00",
    "L01 A00 F20 P10",
    "E10 F21 P11 E11",
    "L10 L11 A10 A11",
    "F30 P20 F31 P21",
    "E20 E21 L20 L21",
    "A20 A21 B10 P30",
    "E30 A01 B11 P31",
    "E31 L30 L31 A30",
    "B20 B21 A31 B30",
    "B00 B01 B31",
)
ORDERS = (ORDER, ORDER, ORDER, ORDER)


def fused_kernel(
    input_hbm,
    pre_hbm,
    post_hbm,
    taps_hbm,
    proj_hbm,
    residual_hbm,
    gain_hbm,
    routes_hbm,
    weight_hbm,
    gate_hbm,
    up_hbm,
    down_hbm,
    out,
    conv_input,
    pre_gate,
    post_gate,
    conv_taps,
    proj,
    residual,
    gain,
    routes,
    route_weight,
    w_gate,
    w_up,
    w_down,
    halo,
    gated,
    mix_out,
    mix_in,
    stream,
    weigh_out,
    weigh,
    leaving,
    tok,
    begun,
    hidden,
    part,
    from_core,
    kept,
    to_chip,
    from_chip,
    to_home,
    home,
    known,
    load_sem,
    sent,
    halo_recv,
    mix_recv,
    weigh_recv,
    z_recv,
    x_recv,
    core_recv,
    one_recv,
    two_recv,
    home_recv,
):
    s, t = lax.axis_index("sp"), lax.axis_index("tp")
    rows, width = residual.shape
    half = width // 2
    channels = conv_input.shape[1]
    cap = rows // GROUPS
    units = w_gate.shape[2]
    core, chip, far = t + 1 - 2 * (t % 2), (t + 2) % 4, 3 - t
    sp_of = [s, s + 1 - 2 * (s % 2), (s + 2) % 4, 3 - s]
    pos = lambda place: (place % 2) * 2 + place // 2
    middle = (s == 1) | (s == 2)
    X_SENT, Z_SENT, ONE_SENT, TWO_SENT, MIX_SENT, WEIGH_SENT, HALO_SENT = range(7)

    def describe(src, dst, group, recv_sem, **where):
        return pltpu.make_async_remote_copy(
            src_ref=src,
            dst_ref=dst,
            send_sem=sent.at[group],
            recv_sem=recv_sem,
            device_id=where,
            device_id_type=pl.DeviceIdType.MESH,
        )

    def send(*refs, **where):
        describe(*refs, **where).start()

    def wait_for(piece, sem):
        pltpu.make_async_copy(piece, piece, sem).wait()

    def signal(sem, **where):
        pl.semaphore_signal(sem, inc=1, device_id=where, device_id_type=pl.DeviceIdType.MESH)

    barrier = pltpu.get_barrier_semaphore()
    signal(barrier, sp=sp_of[1])

    @pl.when(middle)
    def _():
        signal(barrier, sp=sp_of[3])

    for other in (core, chip, far):
        signal(barrier, tp=other)
    loads = []
    for i, (a, b) in enumerate(
        (
            (input_hbm, conv_input),
            (pre_hbm, pre_gate),
            (post_hbm, post_gate),
            (taps_hbm, conv_taps),
            (routes_hbm, routes),
            (weight_hbm, route_weight),
            (gain_hbm, gain),
            (residual_hbm, residual),
            (proj_hbm, proj),
            (gate_hbm, w_gate),
            (up_hbm, w_up),
            (down_hbm, w_down),
        )
    ):
        loads.append(pltpu.make_async_copy(a, b, load_sem.at[i]))
    for load in loads[:7]:
        load.start()
    for load in loads[:4]:
        load.wait()
    for load in loads[7:]:
        load.start()

    count = conv_input.shape[0]
    gated[pl.ds(8, count), :] = pre_gate[...].astype(F32) * conv_input[...].astype(F32)
    taps = conv_taps[:, pl.ds(pl.multiple_of(t * channels, channels), channels)]

    def mix(place, low, size):
        start = pl.multiple_of(place * rows, rows) + low
        g = gated[pl.ds(start, size + 8), :]
        conv = g[8:] * taps[2:3] + g[7:-1] * taps[1:2] + g[6:-2] * taps[0:1]
        return (post_gate[pl.ds(start, size), :].astype(F32) * conv).astype(BF16)

    edge = 16
    partners = (chip, far, core)

    def send_mixed(i, low, size):
        piece = pl.ds(low, size)
        send(
            mix_out.at[i, piece, :],
            mix_in.at[t, piece, :],
            MIX_SENT,
            mix_recv.at[t],
            tp=partners[i],
        )

    def wait_mixed(place):
        wait_for(mix_in.at[place], mix_recv.at[place])

    gated[0:8, :] = jnp.zeros((8, channels), F32)
    for i in range(3):
        mix_out[i] = mix(partners[i], 0, rows)

    @pl.when(middle)
    def _():
        pl.semaphore_wait(barrier, 5)

    @pl.when(jnp.logical_not(middle))
    def _():
        pl.semaphore_wait(barrier, 4)

    def halo_copy(i):
        ref = (conv_input, pre_gate)[i]
        return describe(
            ref.at[pl.ds(count - 16, 16), :],
            halo.at[i],
            HALO_SENT,
            halo_recv.at[0],
            sp=(s + 1) % 4,
        )

    @pl.when(s < 3)
    def _():
        for i in range(2):
            halo_copy(i).start()

    for i in range(3):

        @pl.when(partners[i] > 0)
        def _():
            send_mixed(i, 0, rows)

        @pl.when(partners[i] == 0)
        def _():
            send_mixed(i, edge, rows - edge)

    @pl.when(middle)
    def _():
        signal(known, sp=sp_of[3])
        signal(known, sp=sp_of[1])

    for load in loads[4:6]:
        load.wait()
    first, second = routes[0:1, :], routes[1:2, :]
    epg = w_gate.shape[0]
    down = lax.broadcasted_iota(jnp.int32, (rows, rows), 0)
    across = lax.broadcasted_iota(jnp.int32, (rows, rows), 1)
    group = lax.broadcasted_iota(jnp.int32, (16, rows), 0)
    member = (first >= group * epg) & (first < group * epg + epg) & (group < GROUPS)
    member = jnp.where(member, 1.0, 0.0)
    earlier = jnp.where(down < across, 1.0, 0.0).astype(BF16)
    rank = dot(member.astype(BF16), earlier)
    slot = jnp.sum(member * (rank + (group * cap).astype(F32)), axis=0, keepdims=True)
    pick = jnp.where(slot == down.astype(F32), 1.0, 0.0)
    back = pick.T.astype(BF16)
    pick = pick.astype(BF16)
    low = jnp.where(first < second, route_weight[0:1, :], route_weight[1:2, :])
    high = jnp.where(first < second, route_weight[1:2, :], route_weight[0:1, :])
    low_top, high_top = low.astype(BF16).astype(F32), high.astype(BF16).astype(F32)
    line = lax.broadcasted_iota(jnp.int32, (LANES, rows), 0)
    scales = jnp.where(
        line == 0,
        low_top,
        jnp.where(
            line == 1,
            low - low_top,
            jnp.where(line == 2, high_top, jnp.where(line == 3, high - high_top, 0.0)),
        ),
    ).astype(BF16)
    scales = lax.dot_general(
        pick, scales, (((1,), (1,)), ((), ())), preferred_element_type=F32
    )
    weigh_out[...] = scales.astype(BF16)

    @pl.when(s > 0)
    def _():
        wait_for(halo, halo_recv.at[0])
        gated[0:8, :] = halo[0, 8:16, :].astype(F32) * halo[1, 8:16, :].astype(F32)

    for i in range(3):

        @pl.when(partners[i] == 0)
        def _():
            mix_out[i, 0:edge, :] = mix(0, 0, edge)
            send_mixed(i, 0, edge)

    mix_in[t] = mix(t, 0, rows)

    @pl.when(middle)
    def _():
        pl.semaphore_wait(known, 1)
        signal(known, sp=sp_of[1])

    group_rows = lambda g: pl.ds(pl.multiple_of(g * cap, cap), cap)
    block = lambda place: pl.ds(pl.multiple_of(pos(place) * cap, cap), cap)
    weigh[s, block(t), :] = weigh_out[group_rows(s), :]

    def forward_weigh():
        wait_for(weigh.at[0:3, 0:cap, :], weigh_recv.at[0])
        for k in range(4):
            mine = weigh.at[sp_of[k], block(t), :]
            src = mine if k else weigh_out.at[group_rows(s), :]
            send(src, mine, WEIGH_SENT, weigh_recv.at[1], tp=chip)
            send(src, mine, WEIGH_SENT, weigh_recv.at[2], tp=core)

    def pass_weigh():
        wait_for(weigh.at[:, 0:cap, :], weigh_recv.at[1])
        for k in range(4):
            arrived = weigh.at[sp_of[k], block(chip), :]
            send(arrived, arrived, WEIGH_SENT, weigh_recv.at[2], tp=core)

    tile = 1024
    tiles = width // tile
    column = lambda n: pl.ds(pl.multiple_of(n * tile, tile), tile)
    weights_of = lambda place: pl.ds(pl.multiple_of(place * channels, channels), channels)
    loads[7].wait()
    loads[8].wait()
    wait_mixed(core)

    def project_near(n, carry):
        cols = column(n)
        total = residual[:, cols].astype(F32)
        for place in (t, core):
            total += dot(mix_in[place], proj[weights_of(place), cols])
        stream[:, cols] = total
        return carry

    lax.fori_loop(0, tiles, project_near, 0)
    wait_mixed(chip)

    def project_chip(n, carry):
        cols = column(n)
        stream[:, cols] += dot(mix_in[chip], proj[weights_of(chip), cols])
        return carry

    lax.fori_loop(0, tiles, project_chip, 0)

    @pl.when(jnp.logical_not(middle))
    def _():
        pl.semaphore_wait(known, 2)

    for k in (1, 2, 3):
        send(
            weigh_out.at[group_rows(sp_of[k]), :],
            weigh.at[s, block(t), :],
            WEIGH_SENT,
            weigh_recv.at[0],
            sp=sp_of[k],
        )
    wait_mixed(far)

    def project_far(n, squares):
        cols = column(n)
        total = stream[:, cols] + dot(mix_in[far], proj[weights_of(far), cols])
        stream[:, cols] = total
        return squares + jnp.sum(total * total, axis=1, keepdims=True)

    squares = lax.fori_loop(0, tiles, project_far, jnp.zeros((rows, 1), F32))
    scale = lax.rsqrt(squares / width + 1e-06)
    loads[6].wait()

    def forward(k, h):
        dst = tok.at[sp_of[k], h, block(t), :]
        src = leaving.at[h, group_rows(s), :]
        if k:
            wait_for(dst, z_recv.at[2 * k + h - 2])
            src = dst
        i = 2 * k + h
        send(src, dst, X_SENT, x_recv.at[i], tp=chip)
        send(src, dst, X_SENT, core_recv.at[i], tp=core)
        if not k:
            tok[s, h, block(t), :] = leaving[h, group_rows(s), :]

    def leave(k, h):
        send(
            leaving.at[h, group_rows(sp_of[k]), :],
            tok.at[s, h, block(t), :],
            Z_SENT,
            z_recv.at[2 * k + h - 2],
            sp=sp_of[k],
        )

    for h in (0, 1):

        def norm(n, carry):
            cols = column(n + h * (tiles // 2))
            row = (stream[:, cols] * scale * gain[:, cols]).astype(BF16)
            leaving[h, :, column(n)] = dot(pick, row).astype(BF16)
            return carry

        lax.fori_loop(0, tiles // 2, norm, 0)
        if h == 0:
            for stage in " ".join(EARLY).split():
                (leave if stage[0] == "Z" else forward)(*map(int, stage[1:]))

    for load in loads[9:]:
        load.wait()

    def pass_on(k, h):
        i = 2 * k + h
        arrived = tok.at[sp_of[k], h, block(chip), :]
        wait_for(arrived, x_recv.at[i])
        send(arrived, arrived, X_SENT, core_recv.at[i], tp=core)

    core_rows = lambda c: pl.ds(pl.multiple_of(c * 2 * cap, cap), 2 * cap)

    def experts(k, h):
        g = sp_of[k]
        wait_for(tok.at[g, h, 0 : 2 * cap, :], core_recv.at[2 * k + h])
        x = tok[g, h]
        deep = pl.ds(h * half, half)
        if h == 0:
            for e in range(epg):
                begun[k, 2 * e] = dot(x, w_gate[e, deep, :])
                begun[k, 2 * e + 1] = dot(x, w_up[e, deep, :])
            return
        top = weigh[g].astype(F32)
        for e in range(epg):
            w = top[:, 2 * e : 2 * e + 1] + top[:, 2 * e + 1 : 2 * e + 2]
            gate = begun[k, 2 * e] + dot(x, w_gate[e, deep, :])
            upper = begun[k, 2 * e + 1] + dot(x, w_up[e, deep, :])
            act = gate / (1.0 + jnp.exp(-gate)) * upper * w
            hidden[k, :, pl.ds(e * units, units)] = act.astype(BF16)

    def lower(k, h):
        def step(n, carry):
            cols = column(n + h * (tiles // 2))
            part[k, h, :, column(n)] = dot(hidden[k], w_down[:, cols]).astype(BF16)
            return carry

        lax.fori_loop(0, tiles // 2, step, 0)
        send(
            part.at[k, h, core_rows(1 - t % 2), :],
            from_core.at[k, h],
            ONE_SENT,
            one_recv.at[2 * k + h],
            tp=core,
        )

    def add_core(k, h):
        i = 2 * k + h
        wait_for(from_core.at[k, h], one_recv.at[i])
        for mine in (False, True):
            x = t // 2 if mine else 1 - t // 2
            base = pl.multiple_of((t % 2) * 2 * cap + x * cap, cap)
            near = pl.multiple_of(x * cap, cap)
            total = part[k, h, pl.ds(base, cap), :].astype(F32)
            total += from_core[k, h, pl.ds(near, cap), :].astype(F32)
            if mine:
                kept[k, h] = total
            else:
                to_chip[k, h] = total.astype(BF16)
                send(
                    to_chip.at[k, h],
                    from_chip.at[k, h],
                    TWO_SENT,
                    two_recv.at[i],
                    tp=chip,
                )

    def add_chip(k, h):
        wait_for(from_chip.at[k, h], two_recv.at[2 * k + h])
        total = (kept[k, h] + from_chip[k, h].astype(F32)).astype(BF16)
        if k == 0:
            home[h, group_rows(s), :] = total
        else:
            to_home[k, h] = total
            send(
                to_home.at[k, h],
                home.at[h, group_rows(s), :],
                Z_SENT,
                home_recv.at[h],
                sp=sp_of[k],
            )

    stages = dict(
        F=forward,
        P=pass_on,
        E=experts,
        L=lower,
        A=add_core,
        B=add_chip,
        W=forward_weigh,
        V=pass_weigh,
        Y=lambda: wait_for(weigh.at[:, 0 : 2 * cap, :], weigh_recv.at[2]),
        Z=leave,
    )
    for order in dict.fromkeys(ORDERS):
        where = [i for i in range(4) if ORDERS[i] == order]

        def run():
            for stage in " ".join(order).split():
                stages[stage[0]](*map(int, stage[1:]))

        if len(where) == 4:
            run()
        else:
            chosen = functools.reduce(jnp.logical_or, [s == i for i in where])
            pl.when(chosen)(run)

    for h in (0, 1):

        def finish(n, carry):
            cols = column(n + h * (tiles // 2))
            out[:, cols] = (stream[:, cols] + dot(back, home[h, :, column(n)])).astype(BF16)
            return carry

        wait_for(home.at[h, 0 : 3 * cap, :], home_recv.at[h])
        lax.fori_loop(0, tiles // 2, finish, 0)
    wait_for(tok.at[0:3], sent.at[X_SENT])
    wait_for(tok.at[0:3, :, 0 : 2 * cap, :], sent.at[Z_SENT])
    wait_for(tok.at[0:2], sent.at[ONE_SENT])
    wait_for(tok.at[0], sent.at[TWO_SENT])
    wait_for(mix_out, sent.at[MIX_SENT])
    wait_for(weigh.at[0:3], sent.at[WEIGH_SENT])
    wait_for(weigh.at[0:3, 0:cap, :], sent.at[WEIGH_SENT])

    @pl.when(s < 3)
    def _():
        wait_for(halo, sent.at[HALO_SENT])


def fused(*args):
    (conv_input, _, _, _, out_proj, residual, gain, _, _, w_gate, w_up, w_down) = args
    rows, width = residual.shape
    count, channels = conv_input.shape
    local, _, units = w_gate.shape
    cap = rows // GROUPS
    half = width // 2
    w_down = w_down.reshape(local * units, width)
    args = args[:6] + (gain.reshape(1, width), args[7].T, args[8].T) + args[9:11] + (w_down,)
    far = pl.BlockSpec(memory_space=pl.ANY)
    vmem, sems = pltpu.VMEM, pltpu.SemaphoreType.DMA
    return pl.pallas_call(
        fused_kernel,
        out_shape=vmem((rows, width), BF16),
        in_specs=[far] * 12,
        out_specs=pl.BlockSpec(memory_space=vmem),
        scratch_shapes=[vmem(arg.shape, arg.dtype) for arg in args]
        + [
            vmem((2, 16, channels), BF16),
            vmem((count + 8, channels), F32),
            vmem((3, rows, channels), BF16),
            vmem((4, rows, channels), BF16),
            vmem((rows, width), F32),
            vmem((rows, LANES), BF16),
            vmem((4, rows, LANES), BF16),
            vmem((2, rows, half), BF16),
            vmem((4, 2, rows, half), BF16),
            vmem((4, 2 * local, rows, units), F32),
            vmem((4, rows, local * units), BF16),
            vmem((4, 2, rows, half), BF16),
            vmem((4, 2, 2 * cap, half), BF16),
            vmem((4, 2, cap, half), F32),
            vmem((4, 2, cap, half), BF16),
            vmem((4, 2, cap, half), BF16),
            vmem((4, 2, cap, half), BF16),
            vmem((2, rows, half), BF16),
            pltpu.SemaphoreType.REGULAR,
        ]
        + [sems((n,)) for n in (12, 7, 1, 4, 3, 6, 8, 8, 8, 8, 2)],
        compiler_params=pltpu.CompilerParams(
            collective_id=0, has_side_effects=True, vmem_limit_bytes=56 << 20
        ),
    )(*args)


def on_device(*args):
    residual, routes, w_gate = args[5], args[7], args[9]
    rows, local, seq_ranks = residual.shape[0], w_gate.shape[0], lax.axis_size("sp")
    dense = local == routes.shape[1] == 2 and local * seq_ranks == local * GROUPS
    if dense and lax.axis_size("tp") == 4 and rows % LANES == 0:
        return fused(*args)
    return generic(*args)


def solution(mesh):
    return jax.shard_map(
        on_device,
        mesh=mesh,
        in_specs=(
            P(("grp", "sp"), "tp"),
            P(("grp", "sp"), "tp"),
            P(("grp", "sp"), "tp"),
            P(),
            P(),
            P(("grp", "sp", "tp"), None),
            P(),
            P(("grp", "sp", "tp"), None),
            P(("grp", "sp", "tp"), None),
            P("sp", None, "tp"),
            P("sp", None, "tp"),
            P("sp", "tp", None),
        ),
        out_specs=P(("grp", "sp", "tp"), None),
        check_vma=False,
    )
```

```python
import functools

import jax
import jax.numpy as jnp
from jax import lax
from jax.experimental import pallas as pl
from jax.experimental.pallas import tpu as pltpu
from jax.sharding import PartitionSpec as P

GROUPS = 4
LANES = 128
F32, BF16 = jnp.float32, jnp.bfloat16


def shifted(block, axis, distance):
    devices = range(lax.axis_size(axis))
    route = [(i - distance, i) for i in devices if i - distance in devices]
    return lax.ppermute(block, axis, route)


def generic(
    conv_input,
    pre_gate,
    post_gate,
    conv_taps,
    out_proj,
    residual_in,
    norm_gain,
    routes,
    route_weight,
    w_gate,
    w_up,
    w_down,
):
    shards = lax.axis_size("tp")
    place = lax.axis_index("tp")
    seq_ranks = lax.axis_size("sp")
    channels = conv_input.shape[1]
    width = residual_in.shape[1]
    taps = lax.dynamic_slice_in_dim(conv_taps, place * channels, channels, 1)
    prior_input, prior_gate = shifted((conv_input[-2:], pre_gate[-2:]), "sp", 1)
    gated = jnp.concatenate(
        [
            prior_gate.astype(jnp.float32) * prior_input.astype(jnp.float32),
            pre_gate.astype(jnp.float32) * conv_input.astype(jnp.float32),
        ],
        axis=0,
    )
    conv = gated[2:] * taps[2] + gated[1:-1] * taps[1] + gated[:-2] * taps[0]
    mixed = (post_gate.astype(jnp.float32) * conv).astype(jnp.bfloat16)
    token_rows = lax.all_to_all(mixed, "tp", split_axis=0, concat_axis=1, tiled=True)
    projected = jnp.dot(token_rows, out_proj, preferred_element_type=jnp.float32)
    stream = residual_in.astype(jnp.float32) + projected
    scale = lax.rsqrt(jnp.mean(stream * stream, axis=-1, keepdims=True) + 1e-06)
    normed = (stream * scale * norm_gain).astype(jnp.bfloat16)
    block_rows = routes.shape[0]
    local_experts = w_gate.shape[0]
    experts = local_experts * seq_ranks
    capacity = 2 * block_rows // experts
    flat_routes = routes.reshape(-1)
    position = jnp.arange(flat_routes.shape[0], dtype=jnp.int32)
    earlier = (flat_routes[:, None] == flat_routes[None, :]) & (
        position[None, :] < position[:, None]
    )
    rank = jnp.sum(earlier.astype(jnp.int32), axis=1)
    slot = flat_routes * capacity + rank
    outgoing = (
        jnp.zeros((experts * capacity, width), jnp.bfloat16).at[slot].set(normed[position // 2])
    )
    outgoing = outgoing.reshape(seq_ranks, local_experts, capacity, width)
    spread = lax.all_gather(
        lax.all_to_all(outgoing, "sp", split_axis=0, concat_axis=0, tiled=True)[:, None],
        "tp",
        axis=1,
        tiled=True,
    )
    count = spread.shape[3]
    partials = []
    for expert in range(local_experts):
        rows = spread[:, :, expert].reshape(seq_ranks * shards * count, width)
        gate = jnp.dot(rows, w_gate[expert], preferred_element_type=jnp.float32)
        upper = jnp.dot(rows, w_up[expert], preferred_element_type=jnp.float32)
        hidden = (jax.nn.silu(gate) * upper).astype(jnp.bfloat16)
        part = jnp.dot(hidden, w_down[expert], preferred_element_type=jnp.float32).astype(
            jnp.bfloat16
        )
        partials.append(part.reshape(seq_ranks, shards, count, width))
    stacked = jnp.stack(partials, axis=2)
    summed = lax.psum_scatter(stacked, "tp", scatter_dimension=1, tiled=True).astype(jnp.float32)
    returned = lax.all_to_all(
        summed[:, 0].astype(jnp.bfloat16), "sp", split_axis=0, concat_axis=0, tiled=True
    )
    results = returned.reshape(experts * capacity, width)[slot]
    results = results.reshape(block_rows, 2, width).astype(jnp.float32)
    weighted = jnp.sum(route_weight[:, :, None] * results, axis=1)
    return (stream + weighted).astype(jnp.bfloat16)


def dot(a, b):
    return jnp.dot(a, b, preferred_element_type=F32)


EARLY = ("Z10 F00",)
ORDER = (
    "Z11 Z20 Z21 Z30",
    "Z31 F01 W P00",
    "F10 E00 V P01",
    "F11 Y E01 L00",
    "L01 F20 P10 E10",
    "A00 F21 P11 E11",
    "L10 L11 F30 P20",
    "E20 F31 A10 P21",
    "E21 P30 L20 L21",
    "E30 A20 A21 P31",
    "A11 E31 L30 L31",
    "B10 B20 A30 A31",
    "B21 A01 B11 B30",
    "B31 B00 B01",
)
ORDERS = (ORDER, ORDER, ORDER, ORDER)


def fused_kernel(
    input_hbm,
    pre_hbm,
    post_hbm,
    taps_hbm,
    proj_hbm,
    residual_hbm,
    gain_hbm,
    routes_hbm,
    weight_hbm,
    gate_hbm,
    up_hbm,
    down_hbm,
    out,
    conv_input,
    pre_gate,
    post_gate,
    conv_taps,
    proj,
    residual,
    gain,
    routes,
    route_weight,
    w_gate,
    w_up,
    w_down,
    halo,
    gated,
    mix_out,
    mix_in,
    stream,
    weigh_out,
    weigh,
    leaving,
    tok,
    begun,
    hidden,
    part,
    from_core,
    kept,
    to_chip,
    from_chip,
    to_home,
    home,
    known,
    load_sem,
    sent,
    halo_recv,
    mix_recv,
    weigh_recv,
    z_recv,
    x_recv,
    core_recv,
    one_recv,
    two_recv,
    home_recv,
):
    s, t = lax.axis_index("sp"), lax.axis_index("tp")
    rows, width = residual.shape
    half = width // 2
    channels = conv_input.shape[1]
    cap = rows // GROUPS
    units = w_gate.shape[2]
    core, chip, far = t + 1 - 2 * (t % 2), (t + 2) % 4, 3 - t
    sp_of = [s, s + 1 - 2 * (s % 2), (s + 2) % 4, 3 - s]
    pos = lambda place: (place % 2) * 2 + place // 2
    middle = (s == 1) | (s == 2)
    X_SENT, Z_SENT, ONE_SENT, TWO_SENT, MIX_SENT, WEIGH_SENT, HALO_SENT = range(7)

    def describe(src, dst, group, recv_sem, **where):
        return pltpu.make_async_remote_copy(
            src_ref=src,
            dst_ref=dst,
            send_sem=sent.at[group],
            recv_sem=recv_sem,
            device_id=where,
            device_id_type=pl.DeviceIdType.MESH,
        )

    def send(*refs, **where):
        describe(*refs, **where).start()

    def wait_for(piece, sem):
        pltpu.make_async_copy(piece, piece, sem).wait()

    def signal(sem, **where):
        pl.semaphore_signal(sem, inc=1, device_id=where, device_id_type=pl.DeviceIdType.MESH)

    barrier = pltpu.get_barrier_semaphore()
    signal(barrier, sp=sp_of[1])

    @pl.when(middle)
    def _():
        signal(barrier, sp=sp_of[3])

    for other in (core, chip, far):
        signal(barrier, tp=other)
    loads = []
    for i, (a, b) in enumerate(
        (
            (input_hbm, conv_input),
            (pre_hbm, pre_gate),
            (post_hbm, post_gate),
            (taps_hbm, conv_taps),
            (routes_hbm, routes),
            (weight_hbm, route_weight),
            (gain_hbm, gain),
            (residual_hbm, residual),
            (proj_hbm, proj),
            (gate_hbm, w_gate),
            (up_hbm, w_up),
            (down_hbm, w_down),
        )
    ):
        loads.append(pltpu.make_async_copy(a, b, load_sem.at[i]))
    for load in loads[:7]:
        load.start()
    for load in loads[:4]:
        load.wait()
    for load in loads[7:]:
        load.start()

    count = conv_input.shape[0]
    gated[pl.ds(8, count), :] = pre_gate[...].astype(F32) * conv_input[...].astype(F32)
    taps = conv_taps[:, pl.ds(pl.multiple_of(t * channels, channels), channels)]

    def mix(place, low, size):
        start = pl.multiple_of(place * rows, rows) + low
        g = gated[pl.ds(start, size + 8), :]
        conv = g[8:] * taps[2:3] + g[7:-1] * taps[1:2] + g[6:-2] * taps[0:1]
        return (post_gate[pl.ds(start, size), :].astype(F32) * conv).astype(BF16)

    edge = 16
    partners = (chip, far, core)

    def send_mixed(i, low, size):
        piece = pl.ds(low, size)
        send(
            mix_out.at[i, piece, :],
            mix_in.at[t, piece, :],
            MIX_SENT,
            mix_recv.at[t],
            tp=partners[i],
        )

    def wait_mixed(place):
        wait_for(mix_in.at[place], mix_recv.at[place])

    gated[0:8, :] = jnp.zeros((8, channels), F32)
    for i in range(3):
        mix_out[i] = mix(partners[i], 0, rows)

    @pl.when(middle)
    def _():
        pl.semaphore_wait(barrier, 5)

    @pl.when(jnp.logical_not(middle))
    def _():
        pl.semaphore_wait(barrier, 4)

    def halo_copy(i):
        ref = (conv_input, pre_gate)[i]
        return describe(
            ref.at[pl.ds(count - 16, 16), :],
            halo.at[i],
            HALO_SENT,
            halo_recv.at[0],
            sp=(s + 1) % 4,
        )

    @pl.when(s < 3)
    def _():
        for i in range(2):
            halo_copy(i).start()

    for i in range(3):

        @pl.when(partners[i] > 0)
        def _():
            send_mixed(i, 0, rows)

        @pl.when(partners[i] == 0)
        def _():
            send_mixed(i, edge, rows - edge)

    @pl.when(middle)
    def _():
        signal(known, sp=sp_of[3])
        signal(known, sp=sp_of[1])

    for load in loads[4:6]:
        load.wait()
    first, second = routes[0:1, :], routes[1:2, :]
    epg = w_gate.shape[0]
    down = lax.broadcasted_iota(jnp.int32, (rows, rows), 0)
    across = lax.broadcasted_iota(jnp.int32, (rows, rows), 1)
    group = lax.broadcasted_iota(jnp.int32, (16, rows), 0)
    member = (first >= group * epg) & (first < group * epg + epg) & (group < GROUPS)
    member = jnp.where(member, 1.0, 0.0)
    earlier = jnp.where(down < across, 1.0, 0.0).astype(BF16)
    rank = dot(member.astype(BF16), earlier)
    slot = jnp.sum(member * (rank + (group * cap).astype(F32)), axis=0, keepdims=True)
    pick = jnp.where(slot == down.astype(F32), 1.0, 0.0)
    back = pick.T.astype(BF16)
    pick = pick.astype(BF16)
    low = jnp.where(first < second, route_weight[0:1, :], route_weight[1:2, :])
    high = jnp.where(first < second, route_weight[1:2, :], route_weight[0:1, :])
    low_top, high_top = low.astype(BF16).astype(F32), high.astype(BF16).astype(F32)
    line = lax.broadcasted_iota(jnp.int32, (LANES, rows), 0)
    scales = jnp.where(
        line == 0,
        low_top,
        jnp.where(
            line == 1,
            low - low_top,
            jnp.where(line == 2, high_top, jnp.where(line == 3, high - high_top, 0.0)),
        ),
    ).astype(BF16)
    scales = lax.dot_general(
        pick, scales, (((1,), (1,)), ((), ())), preferred_element_type=F32
    )
    weigh_out[...] = scales.astype(BF16)

    group_rows = lambda g: pl.ds(pl.multiple_of(g * cap, cap), cap)
    block = lambda place: pl.ds(pl.multiple_of(pos(place) * cap, cap), cap)

    def send_weigh(*others):
        for k in others:
            send(
                weigh_out.at[group_rows(sp_of[k]), :],
                weigh.at[s, block(t), :],
                WEIGH_SENT,
                weigh_recv.at[0],
                sp=sp_of[k],
            )

    @pl.when(middle)
    def _():
        send_weigh(1, 3)
        pl.semaphore_wait(known, 1)
        signal(known, sp=sp_of[1])
        send_weigh(2)

    @pl.when(s == 3)
    def _():
        pl.semaphore_wait(known, 2)
        send_weigh(1, 2, 3)

    @pl.when(s > 0)
    def _():
        wait_for(halo, halo_recv.at[0])
        gated[0:8, :] = halo[0, 8:16, :].astype(F32) * halo[1, 8:16, :].astype(F32)

    for i in range(3):

        @pl.when(partners[i] == 0)
        def _():
            mix_out[i, 0:edge, :] = mix(0, 0, edge)
            send_mixed(i, 0, edge)

    mix_in[t] = mix(t, 0, rows)


    weigh[s, block(t), :] = weigh_out[group_rows(s), :]

    def forward_weigh():
        wait_for(weigh.at[0:3, 0:cap, :], weigh_recv.at[0])
        for k in range(4):
            mine = weigh.at[sp_of[k], block(t), :]
            src = mine if k else weigh_out.at[group_rows(s), :]
            send(src, mine, WEIGH_SENT, weigh_recv.at[1], tp=chip)
            send(src, mine, WEIGH_SENT, weigh_recv.at[2], tp=core)

    def pass_weigh():
        wait_for(weigh.at[:, 0:cap, :], weigh_recv.at[1])
        for k in range(4):
            arrived = weigh.at[sp_of[k], block(chip), :]
            send(arrived, arrived, WEIGH_SENT, weigh_recv.at[2], tp=core)

    tile = 1024
    tiles = width // tile
    column = lambda n: pl.ds(pl.multiple_of(n * tile, tile), tile)
    weights_of = lambda place: pl.ds(pl.multiple_of(place * channels, channels), channels)
    loads[7].wait()
    loads[8].wait()
    wait_mixed(core)

    def project_near(n, carry):
        cols = column(n)
        total = residual[:, cols].astype(F32)
        for place in (t, core):
            total += dot(mix_in[place], proj[weights_of(place), cols])
        stream[:, cols] = total
        return carry

    lax.fori_loop(0, tiles, project_near, 0)

    @pl.when(s == 0)
    def _():
        pl.semaphore_wait(known, 2)
        send_weigh(1, 2, 3)

    wait_mixed(chip)

    def project_chip(n, carry):
        cols = column(n)
        stream[:, cols] += dot(mix_in[chip], proj[weights_of(chip), cols])
        return carry

    lax.fori_loop(0, tiles, project_chip, 0)
    wait_mixed(far)

    def project_far(n, squares):
        cols = column(n)
        total = stream[:, cols] + dot(mix_in[far], proj[weights_of(far), cols])
        stream[:, cols] = total
        return squares + jnp.sum(total * total, axis=1, keepdims=True)

    squares = lax.fori_loop(0, tiles, project_far, jnp.zeros((rows, 1), F32))
    scale = lax.rsqrt(squares / width + 1e-06)
    loads[6].wait()

    def forward(k, h):
        dst = tok.at[sp_of[k], h, block(t), :]
        src = leaving.at[h, group_rows(s), :]
        if k:
            wait_for(dst, z_recv.at[2 * k + h - 2])
            src = dst
        i = 2 * k + h
        send(src, dst, X_SENT, x_recv.at[i], tp=chip)
        send(src, dst, X_SENT, core_recv.at[i], tp=core)
        if not k:
            tok[s, h, block(t), :] = leaving[h, group_rows(s), :]

    def leave(k, h):
        send(
            leaving.at[h, group_rows(sp_of[k]), :],
            tok.at[s, h, block(t), :],
            Z_SENT,
            z_recv.at[2 * k + h - 2],
            sp=sp_of[k],
        )

    for h in (0, 1):

        def norm(n, carry):
            cols = column(n + h * (tiles // 2))
            row = (stream[:, cols] * scale * gain[:, cols]).astype(BF16)
            leaving[h, :, column(n)] = dot(pick, row).astype(BF16)
            return carry

        lax.fori_loop(0, tiles // 2, norm, 0)
        if h == 0:
            for stage in " ".join(EARLY).split():
                (leave if stage[0] == "Z" else forward)(*map(int, stage[1:]))

    for load in loads[9:]:
        load.wait()

    def pass_on(k, h):
        i = 2 * k + h
        arrived = tok.at[sp_of[k], h, block(chip), :]
        wait_for(arrived, x_recv.at[i])
        send(arrived, arrived, X_SENT, core_recv.at[i], tp=core)

    core_rows = lambda c: pl.ds(pl.multiple_of(c * 2 * cap, cap), 2 * cap)

    def experts(k, h):
        g = sp_of[k]
        wait_for(tok.at[g, h, 0 : 2 * cap, :], core_recv.at[2 * k + h])
        x = tok[g, h]
        deep = pl.ds(h * half, half)
        if h == 0:
            for e in range(epg):
                begun[k, 2 * e] = dot(x, w_gate[e, deep, :])
                begun[k, 2 * e + 1] = dot(x, w_up[e, deep, :])
            return
        top = weigh[g].astype(F32)
        for e in range(epg):
            w = top[:, 2 * e : 2 * e + 1] + top[:, 2 * e + 1 : 2 * e + 2]
            gate = begun[k, 2 * e] + dot(x, w_gate[e, deep, :])
            upper = begun[k, 2 * e + 1] + dot(x, w_up[e, deep, :])
            act = gate / (1.0 + jnp.exp(-gate)) * upper * w
            hidden[k, :, pl.ds(e * units, units)] = act.astype(BF16)

    def lower(k, h):
        def step(n, carry):
            cols = column(n + h * (tiles // 2))
            part[k, h, :, column(n)] = dot(hidden[k], w_down[:, cols]).astype(BF16)
            return carry

        lax.fori_loop(0, tiles // 2, step, 0)
        send(
            part.at[k, h, core_rows(1 - t % 2), :],
            from_core.at[k, h],
            ONE_SENT,
            one_recv.at[2 * k + h],
            tp=core,
        )

    def add_core(k, h):
        i = 2 * k + h
        wait_for(from_core.at[k, h], one_recv.at[i])
        for mine in (False, True):
            x = t // 2 if mine else 1 - t // 2
            base = pl.multiple_of((t % 2) * 2 * cap + x * cap, cap)
            near = pl.multiple_of(x * cap, cap)
            total = part[k, h, pl.ds(base, cap), :].astype(F32)
            total += from_core[k, h, pl.ds(near, cap), :].astype(F32)
            if mine:
                kept[k, h] = total
            else:
                to_chip[k, h] = total.astype(BF16)
                send(
                    to_chip.at[k, h],
                    from_chip.at[k, h],
                    TWO_SENT,
                    two_recv.at[i],
                    tp=chip,
                )

    def add_chip(k, h):
        wait_for(from_chip.at[k, h], two_recv.at[2 * k + h])
        total = (kept[k, h] + from_chip[k, h].astype(F32)).astype(BF16)
        if k == 0:
            home[h, group_rows(s), :] = total
        else:
            to_home[k, h] = total
            send(
                to_home.at[k, h],
                home.at[h, group_rows(s), :],
                Z_SENT,
                home_recv.at[h],
                sp=sp_of[k],
            )

    stages = dict(
        F=forward,
        P=pass_on,
        E=experts,
        L=lower,
        A=add_core,
        B=add_chip,
        W=forward_weigh,
        V=pass_weigh,
        Y=lambda: wait_for(weigh.at[:, 0 : 2 * cap, :], weigh_recv.at[2]),
        Z=leave,
    )
    for order in dict.fromkeys(ORDERS):
        where = [i for i in range(4) if ORDERS[i] == order]

        def run():
            for stage in " ".join(order).split():
                stages[stage[0]](*map(int, stage[1:]))

        if len(where) == 4:
            run()
        else:
            chosen = functools.reduce(jnp.logical_or, [s == i for i in where])
            pl.when(chosen)(run)

    for h in (0, 1):

        def finish(n, carry):
            cols = column(n + h * (tiles // 2))
            out[:, cols] = (stream[:, cols] + dot(back, home[h, :, column(n)])).astype(BF16)
            return carry

        wait_for(home.at[h, 0 : 3 * cap, :], home_recv.at[h])
        lax.fori_loop(0, tiles // 2, finish, 0)
    wait_for(tok.at[0:3], sent.at[X_SENT])
    wait_for(tok.at[0:3, :, 0 : 2 * cap, :], sent.at[Z_SENT])
    wait_for(tok.at[0:2], sent.at[ONE_SENT])
    wait_for(tok.at[0], sent.at[TWO_SENT])
    wait_for(mix_out, sent.at[MIX_SENT])
    wait_for(weigh.at[0:3], sent.at[WEIGH_SENT])
    wait_for(weigh.at[0:3, 0:cap, :], sent.at[WEIGH_SENT])

    @pl.when(s < 3)
    def _():
        wait_for(halo, sent.at[HALO_SENT])


def fused(*args):
    (conv_input, _, _, _, out_proj, residual, gain, _, _, w_gate, w_up, w_down) = args
    rows, width = residual.shape
    count, channels = conv_input.shape
    local, _, units = w_gate.shape
    cap = rows // GROUPS
    half = width // 2
    w_down = w_down.reshape(local * units, width)
    args = args[:6] + (gain.reshape(1, width), args[7].T, args[8].T) + args[9:11] + (w_down,)
    far = pl.BlockSpec(memory_space=pl.ANY)
    vmem, sems = pltpu.VMEM, pltpu.SemaphoreType.DMA
    return pl.pallas_call(
        fused_kernel,
        out_shape=vmem((rows, width), BF16),
        in_specs=[far] * 12,
        out_specs=pl.BlockSpec(memory_space=vmem),
        scratch_shapes=[vmem(arg.shape, arg.dtype) for arg in args]
        + [
            vmem((2, 16, channels), BF16),
            vmem((count + 8, channels), F32),
            vmem((3, rows, channels), BF16),
            vmem((4, rows, channels), BF16),
            vmem((rows, width), F32),
            vmem((rows, LANES), BF16),
            vmem((4, rows, LANES), BF16),
            vmem((2, rows, half), BF16),
            vmem((4, 2, rows, half), BF16),
            vmem((4, 2 * local, rows, units), F32),
            vmem((4, rows, local * units), BF16),
            vmem((4, 2, rows, half), BF16),
            vmem((4, 2, 2 * cap, half), BF16),
            vmem((4, 2, cap, half), F32),
            vmem((4, 2, cap, half), BF16),
            vmem((4, 2, cap, half), BF16),
            vmem((4, 2, cap, half), BF16),
            vmem((2, rows, half), BF16),
            pltpu.SemaphoreType.REGULAR,
        ]
        + [sems((n,)) for n in (12, 7, 1, 4, 3, 6, 8, 8, 8, 8, 2)],
        compiler_params=pltpu.CompilerParams(
            collective_id=0, has_side_effects=True, vmem_limit_bytes=56 << 20
        ),
    )(*args)


def on_device(*args):
    residual, routes, w_gate = args[5], args[7], args[9]
    rows, local, seq_ranks = residual.shape[0], w_gate.shape[0], lax.axis_size("sp")
    dense = local == routes.shape[1] == 2 and local * seq_ranks == local * GROUPS
    if dense and lax.axis_size("tp") == 4 and rows % LANES == 0:
        return fused(*args)
    return generic(*args)


def solution(mesh):
    return jax.shard_map(
        on_device,
        mesh=mesh,
        in_specs=(
            P(("grp", "sp"), "tp"),
            P(("grp", "sp"), "tp"),
            P(("grp", "sp"), "tp"),
            P(),
            P(),
            P(("grp", "sp", "tp"), None),
            P(),
            P(("grp", "sp", "tp"), None),
            P(("grp", "sp", "tp"), None),
            P("sp", None, "tp"),
            P("sp", None, "tp"),
            P("sp", "tp", None),
        ),
        out_specs=P(("grp", "sp", "tp"), None),
        check_vma=False,
    )
```

```python
import functools

import jax
import jax.numpy as jnp
from jax import lax
from jax.experimental import pallas as pl
from jax.experimental.pallas import tpu as pltpu
from jax.sharding import PartitionSpec as P

GROUPS = 4
LANES = 128
F32, BF16 = jnp.float32, jnp.bfloat16


def shifted(block, axis, distance):
    devices = range(lax.axis_size(axis))
    route = [(i - distance, i) for i in devices if i - distance in devices]
    return lax.ppermute(block, axis, route)


def generic(
    conv_input,
    pre_gate,
    post_gate,
    conv_taps,
    out_proj,
    residual_in,
    norm_gain,
    routes,
    route_weight,
    w_gate,
    w_up,
    w_down,
):
    shards = lax.axis_size("tp")
    place = lax.axis_index("tp")
    seq_ranks = lax.axis_size("sp")
    channels = conv_input.shape[1]
    width = residual_in.shape[1]
    taps = lax.dynamic_slice_in_dim(conv_taps, place * channels, channels, 1)
    prior_input, prior_gate = shifted((conv_input[-2:], pre_gate[-2:]), "sp", 1)
    gated = jnp.concatenate(
        [
            prior_gate.astype(jnp.float32) * prior_input.astype(jnp.float32),
            pre_gate.astype(jnp.float32) * conv_input.astype(jnp.float32),
        ],
        axis=0,
    )
    conv = gated[2:] * taps[2] + gated[1:-1] * taps[1] + gated[:-2] * taps[0]
    mixed = (post_gate.astype(jnp.float32) * conv).astype(jnp.bfloat16)
    token_rows = lax.all_to_all(mixed, "tp", split_axis=0, concat_axis=1, tiled=True)
    projected = jnp.dot(token_rows, out_proj, preferred_element_type=jnp.float32)
    stream = residual_in.astype(jnp.float32) + projected
    scale = lax.rsqrt(jnp.mean(stream * stream, axis=-1, keepdims=True) + 1e-06)
    normed = (stream * scale * norm_gain).astype(jnp.bfloat16)
    block_rows = routes.shape[0]
    local_experts = w_gate.shape[0]
    experts = local_experts * seq_ranks
    capacity = 2 * block_rows // experts
    flat_routes = routes.reshape(-1)
    position = jnp.arange(flat_routes.shape[0], dtype=jnp.int32)
    earlier = (flat_routes[:, None] == flat_routes[None, :]) & (
        position[None, :] < position[:, None]
    )
    rank = jnp.sum(earlier.astype(jnp.int32), axis=1)
    slot = flat_routes * capacity + rank
    outgoing = (
        jnp.zeros((experts * capacity, width), jnp.bfloat16).at[slot].set(normed[position // 2])
    )
    outgoing = outgoing.reshape(seq_ranks, local_experts, capacity, width)
    spread = lax.all_gather(
        lax.all_to_all(outgoing, "sp", split_axis=0, concat_axis=0, tiled=True)[:, None],
        "tp",
        axis=1,
        tiled=True,
    )
    count = spread.shape[3]
    partials = []
    for expert in range(local_experts):
        rows = spread[:, :, expert].reshape(seq_ranks * shards * count, width)
        gate = jnp.dot(rows, w_gate[expert], preferred_element_type=jnp.float32)
        upper = jnp.dot(rows, w_up[expert], preferred_element_type=jnp.float32)
        hidden = (jax.nn.silu(gate) * upper).astype(jnp.bfloat16)
        part = jnp.dot(hidden, w_down[expert], preferred_element_type=jnp.float32).astype(
            jnp.bfloat16
        )
        partials.append(part.reshape(seq_ranks, shards, count, width))
    stacked = jnp.stack(partials, axis=2)
    summed = lax.psum_scatter(stacked, "tp", scatter_dimension=1, tiled=True).astype(jnp.float32)
    returned = lax.all_to_all(
        summed[:, 0].astype(jnp.bfloat16), "sp", split_axis=0, concat_axis=0, tiled=True
    )
    results = returned.reshape(experts * capacity, width)[slot]
    results = results.reshape(block_rows, 2, width).astype(jnp.float32)
    weighted = jnp.sum(route_weight[:, :, None] * results, axis=1)
    return (stream + weighted).astype(jnp.bfloat16)


def dot(a, b):
    return jnp.dot(a, b, preferred_element_type=F32)


EARLY = ("Z20 F00",)
ORDER = (
    "Z21 Z10 Z11 Z30",
    "Z31 F01 W P00",
    "F20 E00 V P01",
    "F21 Y E01 L00",
    "L01 F10 P20 E20",
    "A00 F11 P21 E21",
    "L20 L21 F30 P10",
    "E10 F31 A20 A21",
    "P11 E11 P30 L10",
    "L11 E30 P31 A10",
    "E31 L30 L31 B20",
    "B21 A30 A31 A11",
    "B10 A01 B30 B31",
    "B11 B00 B01",
)
ORDERS = (ORDER, ORDER, ORDER, ORDER)


def fused_kernel(
    input_hbm,
    pre_hbm,
    post_hbm,
    taps_hbm,
    proj_hbm,
    residual_hbm,
    gain_hbm,
    routes_hbm,
    weight_hbm,
    gate_hbm,
    up_hbm,
    down_hbm,
    out,
    conv_input,
    pre_gate,
    post_gate,
    conv_taps,
    proj,
    residual,
    gain,
    routes,
    route_weight,
    w_gate,
    w_up,
    w_down,
    halo,
    gated,
    mix_out,
    mix_in,
    stream,
    weigh_out,
    weigh,
    leaving,
    tok,
    begun,
    hidden,
    part,
    from_core,
    kept,
    to_chip,
    from_chip,
    to_home,
    home,
    known,
    load_sem,
    sent,
    halo_recv,
    mix_recv,
    weigh_recv,
    z_recv,
    x_recv,
    core_recv,
    one_recv,
    two_recv,
    home_recv,
):
    s, t = lax.axis_index("sp"), lax.axis_index("tp")
    rows, width = residual.shape
    half = width // 2
    channels = conv_input.shape[1]
    cap = rows // GROUPS
    units = w_gate.shape[2]
    core, chip, far = t + 1 - 2 * (t % 2), (t + 2) % 4, 3 - t
    sp_of = [s, s + 1 - 2 * (s % 2), (s + 2) % 4, 3 - s]
    pos = lambda place: (place % 2) * 2 + place // 2
    middle = (s == 1) | (s == 2)
    X_SENT, Z_SENT, ONE_SENT, TWO_SENT, MIX_SENT, WEIGH_SENT, HALO_SENT = range(7)

    def describe(src, dst, group, recv_sem, **where):
        return pltpu.make_async_remote_copy(
            src_ref=src,
            dst_ref=dst,
            send_sem=sent.at[group],
            recv_sem=recv_sem,
            device_id=where,
            device_id_type=pl.DeviceIdType.MESH,
        )

    def send(*refs, **where):
        describe(*refs, **where).start()

    def wait_for(piece, sem):
        pltpu.make_async_copy(piece, piece, sem).wait()

    def signal(sem, **where):
        pl.semaphore_signal(sem, inc=1, device_id=where, device_id_type=pl.DeviceIdType.MESH)

    barrier = pltpu.get_barrier_semaphore()
    signal(barrier, sp=sp_of[1])

    @pl.when(middle)
    def _():
        signal(barrier, sp=sp_of[3])

    for other in (core, chip, far):
        signal(barrier, tp=other)
    loads = []
    for i, (a, b) in enumerate(
        (
            (input_hbm, conv_input),
            (pre_hbm, pre_gate),
            (post_hbm, post_gate),
            (taps_hbm, conv_taps),
            (routes_hbm, routes),
            (weight_hbm, route_weight),
            (gain_hbm, gain),
            (residual_hbm, residual),
            (proj_hbm, proj),
            (gate_hbm, w_gate),
            (up_hbm, w_up),
            (down_hbm, w_down),
        )
    ):
        loads.append(pltpu.make_async_copy(a, b, load_sem.at[i]))
    for load in loads[:7]:
        load.start()
    for load in loads[:4]:
        load.wait()
    for load in loads[7:]:
        load.start()

    count = conv_input.shape[0]
    gated[pl.ds(8, count), :] = pre_gate[...].astype(F32) * conv_input[...].astype(F32)
    taps = conv_taps[:, pl.ds(pl.multiple_of(t * channels, channels), channels)]

    def mix(place, low, size):
        start = pl.multiple_of(place * rows, rows) + low
        g = gated[pl.ds(start, size + 8), :]
        conv = g[8:] * taps[2:3] + g[7:-1] * taps[1:2] + g[6:-2] * taps[0:1]
        return (post_gate[pl.ds(start, size), :].astype(F32) * conv).astype(BF16)

    edge = 16
    partners = (chip, far, core)

    def send_mixed(i, low, size):
        piece = pl.ds(low, size)
        send(
            mix_out.at[i, piece, :],
            mix_in.at[t, piece, :],
            MIX_SENT,
            mix_recv.at[t],
            tp=partners[i],
        )

    def wait_mixed(place):
        wait_for(mix_in.at[place], mix_recv.at[place])

    gated[0:8, :] = jnp.zeros((8, channels), F32)
    for i in range(3):
        mix_out[i] = mix(partners[i], 0, rows)

    @pl.when(middle)
    def _():
        pl.semaphore_wait(barrier, 5)

    @pl.when(jnp.logical_not(middle))
    def _():
        pl.semaphore_wait(barrier, 4)

    def halo_copy(i):
        ref = (conv_input, pre_gate)[i]
        return describe(
            ref.at[pl.ds(count - 16, 16), :],
            halo.at[i],
            HALO_SENT,
            halo_recv.at[0],
            sp=(s + 1) % 4,
        )

    @pl.when(s < 3)
    def _():
        for i in range(2):
            halo_copy(i).start()

    for i in range(3):

        @pl.when(partners[i] > 0)
        def _():
            send_mixed(i, 0, rows)

        @pl.when(partners[i] == 0)
        def _():
            send_mixed(i, edge, rows - edge)

    @pl.when(middle)
    def _():
        signal(known, sp=sp_of[3])
        signal(known, sp=sp_of[1])

    for load in loads[4:6]:
        load.wait()
    first, second = routes[0:1, :], routes[1:2, :]
    epg = w_gate.shape[0]
    down = lax.broadcasted_iota(jnp.int32, (rows, rows), 0)
    across = lax.broadcasted_iota(jnp.int32, (rows, rows), 1)
    group = lax.broadcasted_iota(jnp.int32, (16, rows), 0)
    member = (first >= group * epg) & (first < group * epg + epg) & (group < GROUPS)
    member = jnp.where(member, 1.0, 0.0)
    earlier = jnp.where(down < across, 1.0, 0.0).astype(BF16)
    rank = dot(member.astype(BF16), earlier)
    slot = jnp.sum(member * (rank + (group * cap).astype(F32)), axis=0, keepdims=True)
    pick = jnp.where(slot == down.astype(F32), 1.0, 0.0)
    back = pick.T.astype(BF16)
    pick = pick.astype(BF16)
    low = jnp.where(first < second, route_weight[0:1, :], route_weight[1:2, :])
    high = jnp.where(first < second, route_weight[1:2, :], route_weight[0:1, :])
    low_top, high_top = low.astype(BF16).astype(F32), high.astype(BF16).astype(F32)
    line = lax.broadcasted_iota(jnp.int32, (LANES, rows), 0)
    scales = jnp.where(
        line == 0,
        low_top,
        jnp.where(
            line == 1,
            low - low_top,
            jnp.where(line == 2, high_top, jnp.where(line == 3, high - high_top, 0.0)),
        ),
    ).astype(BF16)
    scales = lax.dot_general(
        pick, scales, (((1,), (1,)), ((), ())), preferred_element_type=F32
    )
    weigh_out[...] = scales.astype(BF16)

    group_rows = lambda g: pl.ds(pl.multiple_of(g * cap, cap), cap)
    block = lambda place: pl.ds(pl.multiple_of(pos(place) * cap, cap), cap)

    def send_weigh(*others):
        for k in others:
            send(
                weigh_out.at[group_rows(sp_of[k]), :],
                weigh.at[s, block(t), :],
                WEIGH_SENT,
                weigh_recv.at[0],
                sp=sp_of[k],
            )

    @pl.when(middle)
    def _():
        send_weigh(1, 3)
        pl.semaphore_wait(known, 1)
        signal(known, sp=sp_of[1])
        send_weigh(2)

    @pl.when(s == 3)
    def _():
        pl.semaphore_wait(known, 2)
        send_weigh(1, 2, 3)

    @pl.when(s > 0)
    def _():
        wait_for(halo, halo_recv.at[0])
        gated[0:8, :] = halo[0, 8:16, :].astype(F32) * halo[1, 8:16, :].astype(F32)

    for i in range(3):

        @pl.when(partners[i] == 0)
        def _():
            mix_out[i, 0:edge, :] = mix(0, 0, edge)
            send_mixed(i, 0, edge)

    mix_in[t] = mix(t, 0, rows)


    weigh[s, block(t), :] = weigh_out[group_rows(s), :]

    def forward_weigh():
        wait_for(weigh.at[0:3, 0:cap, :], weigh_recv.at[0])
        for k in range(4):
            mine = weigh.at[sp_of[k], block(t), :]
            src = mine if k else weigh_out.at[group_rows(s), :]
            send(src, mine, WEIGH_SENT, weigh_recv.at[1], tp=chip)
            send(src, mine, WEIGH_SENT, weigh_recv.at[2], tp=core)

    def pass_weigh():
        wait_for(weigh.at[:, 0:cap, :], weigh_recv.at[1])
        for k in range(4):
            arrived = weigh.at[sp_of[k], block(chip), :]
            send(arrived, arrived, WEIGH_SENT, weigh_recv.at[2], tp=core)

    tile = 1024
    tiles = width // tile
    column = lambda n: pl.ds(pl.multiple_of(n * tile, tile), tile)
    weights_of = lambda place: pl.ds(pl.multiple_of(place * channels, channels), channels)
    loads[7].wait()
    loads[8].wait()
    wait_mixed(core)

    def project_near(n, carry):
        cols = column(n)
        total = residual[:, cols].astype(F32)
        for place in (t, core):
            total += dot(mix_in[place], proj[weights_of(place), cols])
        stream[:, cols] = total
        return carry

    lax.fori_loop(0, tiles, project_near, 0)

    @pl.when(s == 0)
    def _():
        pl.semaphore_wait(known, 2)
        send_weigh(1, 2, 3)

    sooner = far + (t % 2) * (chip - far)
    later = chip + far - sooner
    wait_mixed(sooner)

    def project_sooner(n, carry):
        cols = column(n)
        stream[:, cols] += dot(mix_in[sooner], proj[weights_of(sooner), cols])
        return carry

    lax.fori_loop(0, tiles, project_sooner, 0)
    wait_mixed(later)

    def project_later(n, squares):
        cols = column(n)
        total = stream[:, cols] + dot(mix_in[later], proj[weights_of(later), cols])
        stream[:, cols] = total
        return squares + jnp.sum(total * total, axis=1, keepdims=True)

    squares = lax.fori_loop(0, tiles, project_later, jnp.zeros((rows, 1), F32))
    scale = lax.rsqrt(squares / width + 1e-06)
    loads[6].wait()

    def forward(k, h):
        dst = tok.at[sp_of[k], h, block(t), :]
        src = leaving.at[h, group_rows(s), :]
        if k:
            wait_for(dst, z_recv.at[2 * k + h - 2])
            src = dst
        i = 2 * k + h
        send(src, dst, X_SENT, x_recv.at[i], tp=chip)
        send(src, dst, X_SENT, core_recv.at[i], tp=core)
        if not k:
            tok[s, h, block(t), :] = leaving[h, group_rows(s), :]

    def leave(k, h):
        send(
            leaving.at[h, group_rows(sp_of[k]), :],
            tok.at[s, h, block(t), :],
            Z_SENT,
            z_recv.at[2 * k + h - 2],
            sp=sp_of[k],
        )

    for h in (0, 1):

        def norm(n, carry):
            cols = column(n + h * (tiles // 2))
            row = (stream[:, cols] * scale * gain[:, cols]).astype(BF16)
            leaving[h, :, column(n)] = dot(pick, row).astype(BF16)
            return carry

        lax.fori_loop(0, tiles // 2, norm, 0)
        if h == 0:
            for stage in " ".join(EARLY).split():
                (leave if stage[0] == "Z" else forward)(*map(int, stage[1:]))

    for load in loads[9:]:
        load.wait()

    def pass_on(k, h):
        i = 2 * k + h
        arrived = tok.at[sp_of[k], h, block(chip), :]
        wait_for(arrived, x_recv.at[i])
        send(arrived, arrived, X_SENT, core_recv.at[i], tp=core)

    core_rows = lambda c: pl.ds(pl.multiple_of(c * 2 * cap, cap), 2 * cap)

    def experts(k, h):
        g = sp_of[k]
        wait_for(tok.at[g, h, 0 : 2 * cap, :], core_recv.at[2 * k + h])
        x = tok[g, h]
        deep = pl.ds(h * half, half)
        if h == 0:
            for e in range(epg):
                begun[k, 2 * e] = dot(x, w_gate[e, deep, :])
                begun[k, 2 * e + 1] = dot(x, w_up[e, deep, :])
            return
        top = weigh[g].astype(F32)
        for e in range(epg):
            w = top[:, 2 * e : 2 * e + 1] + top[:, 2 * e + 1 : 2 * e + 2]
            gate = begun[k, 2 * e] + dot(x, w_gate[e, deep, :])
            upper = begun[k, 2 * e + 1] + dot(x, w_up[e, deep, :])
            act = gate / (1.0 + jnp.exp(-gate)) * upper * w
            hidden[k, :, pl.ds(e * units, units)] = act.astype(BF16)

    def lower(k, h):
        def step(n, carry):
            cols = column(n + h * (tiles // 2))
            part[k, h, :, column(n)] = dot(hidden[k], w_down[:, cols]).astype(BF16)
            return carry

        lax.fori_loop(0, tiles // 2, step, 0)
        send(
            part.at[k, h, core_rows(1 - t % 2), :],
            from_core.at[k, h],
            ONE_SENT,
            one_recv.at[2 * k + h],
            tp=core,
        )

    def add_core(k, h):
        i = 2 * k + h
        wait_for(from_core.at[k, h], one_recv.at[i])
        for mine in (False, True):
            x = t // 2 if mine else 1 - t // 2
            base = pl.multiple_of((t % 2) * 2 * cap + x * cap, cap)
            near = pl.multiple_of(x * cap, cap)
            total = part[k, h, pl.ds(base, cap), :].astype(F32)
            total += from_core[k, h, pl.ds(near, cap), :].astype(F32)
            if mine:
                kept[k, h] = total
            else:
                to_chip[k, h] = total.astype(BF16)
                send(
                    to_chip.at[k, h],
                    from_chip.at[k, h],
                    TWO_SENT,
                    two_recv.at[i],
                    tp=chip,
                )

    def add_chip(k, h):
        wait_for(from_chip.at[k, h], two_recv.at[2 * k + h])
        total = (kept[k, h] + from_chip[k, h].astype(F32)).astype(BF16)
        if k == 0:
            home[h, group_rows(s), :] = total
        else:
            to_home[k, h] = total
            send(
                to_home.at[k, h],
                home.at[h, group_rows(s), :],
                Z_SENT,
                home_recv.at[h],
                sp=sp_of[k],
            )

    stages = dict(
        F=forward,
        P=pass_on,
        E=experts,
        L=lower,
        A=add_core,
        B=add_chip,
        W=forward_weigh,
        V=pass_weigh,
        Y=lambda: wait_for(weigh.at[:, 0 : 2 * cap, :], weigh_recv.at[2]),
        Z=leave,
    )
    for order in dict.fromkeys(ORDERS):
        where = [i for i in range(4) if ORDERS[i] == order]

        def run():
            for stage in " ".join(order).split():
                stages[stage[0]](*map(int, stage[1:]))

        if len(where) == 4:
            run()
        else:
            chosen = functools.reduce(jnp.logical_or, [s == i for i in where])
            pl.when(chosen)(run)

    for h in (0, 1):

        def finish(n, carry):
            cols = column(n + h * (tiles // 2))
            out[:, cols] = (stream[:, cols] + dot(back, home[h, :, column(n)])).astype(BF16)
            return carry

        wait_for(home.at[h, 0 : 3 * cap, :], home_recv.at[h])
        lax.fori_loop(0, tiles // 2, finish, 0)
    wait_for(tok.at[0:3], sent.at[X_SENT])
    wait_for(tok.at[0:3, :, 0 : 2 * cap, :], sent.at[Z_SENT])
    wait_for(tok.at[0:2], sent.at[ONE_SENT])
    wait_for(tok.at[0], sent.at[TWO_SENT])
    wait_for(mix_out, sent.at[MIX_SENT])
    wait_for(weigh.at[0:3], sent.at[WEIGH_SENT])
    wait_for(weigh.at[0:3, 0:cap, :], sent.at[WEIGH_SENT])

    @pl.when(s < 3)
    def _():
        wait_for(halo, sent.at[HALO_SENT])


def fused(*args):
    (conv_input, _, _, _, out_proj, residual, gain, _, _, w_gate, w_up, w_down) = args
    rows, width = residual.shape
    count, channels = conv_input.shape
    local, _, units = w_gate.shape
    cap = rows // GROUPS
    half = width // 2
    w_down = w_down.reshape(local * units, width)
    args = args[:6] + (gain.reshape(1, width), args[7].T, args[8].T) + args[9:11] + (w_down,)
    far = pl.BlockSpec(memory_space=pl.ANY)
    vmem, sems = pltpu.VMEM, pltpu.SemaphoreType.DMA
    return pl.pallas_call(
        fused_kernel,
        out_shape=vmem((rows, width), BF16),
        in_specs=[far] * 12,
        out_specs=pl.BlockSpec(memory_space=vmem),
        scratch_shapes=[vmem(arg.shape, arg.dtype) for arg in args]
        + [
            vmem((2, 16, channels), BF16),
            vmem((count + 8, channels), F32),
            vmem((3, rows, channels), BF16),
            vmem((4, rows, channels), BF16),
            vmem((rows, width), F32),
            vmem((rows, LANES), BF16),
            vmem((4, rows, LANES), BF16),
            vmem((2, rows, half), BF16),
            vmem((4, 2, rows, half), BF16),
            vmem((4, 2 * local, rows, units), F32),
            vmem((4, rows, local * units), BF16),
            vmem((4, 2, rows, half), BF16),
            vmem((4, 2, 2 * cap, half), BF16),
            vmem((4, 2, cap, half), F32),
            vmem((4, 2, cap, half), BF16),
            vmem((4, 2, cap, half), BF16),
            vmem((4, 2, cap, half), BF16),
            vmem((2, rows, half), BF16),
            pltpu.SemaphoreType.REGULAR,
        ]
        + [sems((n,)) for n in (12, 7, 1, 4, 3, 6, 8, 8, 8, 8, 2)],
        compiler_params=pltpu.CompilerParams(
            collective_id=0, has_side_effects=True, vmem_limit_bytes=56 << 20
        ),
    )(*args)


def on_device(*args):
    residual, routes, w_gate = args[5], args[7], args[9]
    rows, local, seq_ranks = residual.shape[0], w_gate.shape[0], lax.axis_size("sp")
    dense = local == routes.shape[1] == 2 and local * seq_ranks == local * GROUPS
    if dense and lax.axis_size("tp") == 4 and rows % LANES == 0:
        return fused(*args)
    return generic(*args)


def solution(mesh):
    return jax.shard_map(
        on_device,
        mesh=mesh,
        in_specs=(
            P(("grp", "sp"), "tp"),
            P(("grp", "sp"), "tp"),
            P(("grp", "sp"), "tp"),
            P(),
            P(),
            P(("grp", "sp", "tp"), None),
            P(),
            P(("grp", "sp", "tp"), None),
            P(("grp", "sp", "tp"), None),
            P("sp", None, "tp"),
            P("sp", None, "tp"),
            P("sp", "tp", None),
        ),
        out_specs=P(("grp", "sp", "tp"), None),
        check_vma=False,
    )
```

```python
import functools

import jax
import jax.numpy as jnp
from jax import lax
from jax.experimental import pallas as pl
from jax.experimental.pallas import tpu as pltpu
from jax.sharding import PartitionSpec as P

GROUPS = 4
LANES = 128
F32, BF16 = jnp.float32, jnp.bfloat16


def shifted(block, axis, distance):
    devices = range(lax.axis_size(axis))
    route = [(i - distance, i) for i in devices if i - distance in devices]
    return lax.ppermute(block, axis, route)


def generic(
    conv_input,
    pre_gate,
    post_gate,
    conv_taps,
    out_proj,
    residual_in,
    norm_gain,
    routes,
    route_weight,
    w_gate,
    w_up,
    w_down,
):
    shards = lax.axis_size("tp")
    place = lax.axis_index("tp")
    seq_ranks = lax.axis_size("sp")
    channels = conv_input.shape[1]
    width = residual_in.shape[1]
    taps = lax.dynamic_slice_in_dim(conv_taps, place * channels, channels, 1)
    prior_input, prior_gate = shifted((conv_input[-2:], pre_gate[-2:]), "sp", 1)
    gated = jnp.concatenate(
        [
            prior_gate.astype(jnp.float32) * prior_input.astype(jnp.float32),
            pre_gate.astype(jnp.float32) * conv_input.astype(jnp.float32),
        ],
        axis=0,
    )
    conv = gated[2:] * taps[2] + gated[1:-1] * taps[1] + gated[:-2] * taps[0]
    mixed = (post_gate.astype(jnp.float32) * conv).astype(jnp.bfloat16)
    token_rows = lax.all_to_all(mixed, "tp", split_axis=0, concat_axis=1, tiled=True)
    projected = jnp.dot(token_rows, out_proj, preferred_element_type=jnp.float32)
    stream = residual_in.astype(jnp.float32) + projected
    scale = lax.rsqrt(jnp.mean(stream * stream, axis=-1, keepdims=True) + 1e-06)
    normed = (stream * scale * norm_gain).astype(jnp.bfloat16)
    block_rows = routes.shape[0]
    local_experts = w_gate.shape[0]
    experts = local_experts * seq_ranks
    capacity = 2 * block_rows // experts
    flat_routes = routes.reshape(-1)
    position = jnp.arange(flat_routes.shape[0], dtype=jnp.int32)
    earlier = (flat_routes[:, None] == flat_routes[None, :]) & (
        position[None, :] < position[:, None]
    )
    rank = jnp.sum(earlier.astype(jnp.int32), axis=1)
    slot = flat_routes * capacity + rank
    outgoing = (
        jnp.zeros((experts * capacity, width), jnp.bfloat16).at[slot].set(normed[position // 2])
    )
    outgoing = outgoing.reshape(seq_ranks, local_experts, capacity, width)
    spread = lax.all_gather(
        lax.all_to_all(outgoing, "sp", split_axis=0, concat_axis=0, tiled=True)[:, None],
        "tp",
        axis=1,
        tiled=True,
    )
    count = spread.shape[3]
    partials = []
    for expert in range(local_experts):
        rows = spread[:, :, expert].reshape(seq_ranks * shards * count, width)
        gate = jnp.dot(rows, w_gate[expert], preferred_element_type=jnp.float32)
        upper = jnp.dot(rows, w_up[expert], preferred_element_type=jnp.float32)
        hidden = (jax.nn.silu(gate) * upper).astype(jnp.bfloat16)
        part = jnp.dot(hidden, w_down[expert], preferred_element_type=jnp.float32).astype(
            jnp.bfloat16
        )
        partials.append(part.reshape(seq_ranks, shards, count, width))
    stacked = jnp.stack(partials, axis=2)
    summed = lax.psum_scatter(stacked, "tp", scatter_dimension=1, tiled=True).astype(jnp.float32)
    returned = lax.all_to_all(
        summed[:, 0].astype(jnp.bfloat16), "sp", split_axis=0, concat_axis=0, tiled=True
    )
    results = returned.reshape(experts * capacity, width)[slot]
    results = results.reshape(block_rows, 2, width).astype(jnp.float32)
    weighted = jnp.sum(route_weight[:, :, None] * results, axis=1)
    return (stream + weighted).astype(jnp.bfloat16)


def dot(a, b):
    return jnp.dot(a, b, preferred_element_type=F32)


EARLY = ("Z20 F00",)
ORDER = (
    "Z21 Z10 Z11 Z30",
    "Z31 F01 W P00",
    "F20 E00 V P01",
    "F21 Y E01 L00",
    "L01 F10 P20 E20",
    "A00 F11 P21 E21",
    "L20 L21 F30 P10",
    "E10 F31 A20 A21",
    "P11 E11 P30 L10",
    "L11 E30 P31 A10",
    "A11 E31 L30 L31",
    "B20 B21 A30 A31",
    "B10 A01 B30 B31",
    "B11 B00 B01",
)
ORDERS = (ORDER, ORDER, ORDER, ORDER)


def fused_kernel(
    input_hbm,
    pre_hbm,
    post_hbm,
    taps_hbm,
    proj_hbm,
    residual_hbm,
    gain_hbm,
    routes_hbm,
    weight_hbm,
    gate_hbm,
    up_hbm,
    down_hbm,
    out,
    conv_input,
    pre_gate,
    post_gate,
    conv_taps,
    proj,
    residual,
    gain,
    routes,
    route_weight,
    w_gate,
    w_up,
    w_down,
    halo,
    gated,
    mix_out,
    mix_in,
    stream,
    weigh_out,
    weigh,
    leaving,
    tok,
    begun,
    hidden,
    part,
    from_core,
    kept,
    to_chip,
    from_chip,
    to_home,
    home,
    known,
    load_sem,
    sent,
    halo_recv,
    mix_recv,
    weigh_recv,
    z_recv,
    x_recv,
    core_recv,
    one_recv,
    two_recv,
    home_recv,
):
    s, t = lax.axis_index("sp"), lax.axis_index("tp")
    rows, width = residual.shape
    half = width // 2
    channels = conv_input.shape[1]
    cap = rows // GROUPS
    units = w_gate.shape[2]
    core, chip, far = t + 1 - 2 * (t % 2), (t + 2) % 4, 3 - t
    sp_of = [s, s + 1 - 2 * (s % 2), (s + 2) % 4, 3 - s]
    pos = lambda place: (place % 2) * 2 + place // 2
    middle = (s == 1) | (s == 2)
    X_SENT, Z_SENT, ONE_SENT, TWO_SENT, MIX_SENT, WEIGH_SENT, HALO_SENT = range(7)

    def describe(src, dst, group, recv_sem, **where):
        return pltpu.make_async_remote_copy(
            src_ref=src,
            dst_ref=dst,
            send_sem=sent.at[group],
            recv_sem=recv_sem,
            device_id=where,
            device_id_type=pl.DeviceIdType.MESH,
        )

    def send(*refs, **where):
        describe(*refs, **where).start()

    def wait_for(piece, sem):
        pltpu.make_async_copy(piece, piece, sem).wait()

    def signal(sem, **where):
        pl.semaphore_signal(sem, inc=1, device_id=where, device_id_type=pl.DeviceIdType.MESH)

    barrier = pltpu.get_barrier_semaphore()
    signal(barrier, sp=sp_of[1])

    @pl.when(middle)
    def _():
        signal(barrier, sp=sp_of[3])

    for other in (core, chip, far):
        signal(barrier, tp=other)
    loads = []
    for i, (a, b) in enumerate(
        (
            (input_hbm, conv_input),
            (pre_hbm, pre_gate),
            (post_hbm, post_gate),
            (taps_hbm, conv_taps),
            (routes_hbm, routes),
            (weight_hbm, route_weight),
            (gain_hbm, gain),
            (residual_hbm, residual),
            (proj_hbm, proj),
            (gate_hbm, w_gate),
            (up_hbm, w_up),
            (down_hbm, w_down),
        )
    ):
        loads.append(pltpu.make_async_copy(a, b, load_sem.at[i]))
    for load in loads[:7]:
        load.start()
    for load in loads[:4]:
        load.wait()
    for load in loads[7:]:
        load.start()

    count = conv_input.shape[0]
    gated[pl.ds(8, count), :] = pre_gate[...].astype(F32) * conv_input[...].astype(F32)
    taps = conv_taps[:, pl.ds(pl.multiple_of(t * channels, channels), channels)]

    def mix(place, low, size):
        start = pl.multiple_of(place * rows, rows) + low
        g = gated[pl.ds(start, size + 8), :]
        conv = g[8:] * taps[2:3] + g[7:-1] * taps[1:2] + g[6:-2] * taps[0:1]
        return (post_gate[pl.ds(start, size), :].astype(F32) * conv).astype(BF16)

    edge = 16
    partners = (chip, far, core)

    def send_mixed(i, low, size):
        piece = pl.ds(low, size)
        send(
            mix_out.at[i, piece, :],
            mix_in.at[t, piece, :],
            MIX_SENT,
            mix_recv.at[t],
            tp=partners[i],
        )

    def wait_mixed(place):
        wait_for(mix_in.at[place], mix_recv.at[place])

    gated[0:8, :] = jnp.zeros((8, channels), F32)
    for i in range(3):
        mix_out[i] = mix(partners[i], 0, rows)

    @pl.when(middle)
    def _():
        pl.semaphore_wait(barrier, 5)

    @pl.when(jnp.logical_not(middle))
    def _():
        pl.semaphore_wait(barrier, 4)

    def halo_copy(i):
        ref = (conv_input, pre_gate)[i]
        return describe(
            ref.at[pl.ds(count - 16, 16), :],
            halo.at[i],
            HALO_SENT,
            halo_recv.at[0],
            sp=(s + 1) % 4,
        )

    @pl.when(s < 3)
    def _():
        for i in range(2):
            halo_copy(i).start()

    for i in range(3):

        @pl.when(partners[i] > 0)
        def _():
            send_mixed(i, 0, rows)

        @pl.when(partners[i] == 0)
        def _():
            send_mixed(i, edge, rows - edge)

    @pl.when(middle)
    def _():
        signal(known, sp=sp_of[3])
        signal(known, sp=sp_of[1])

    for load in loads[4:6]:
        load.wait()
    first, second = routes[0:1, :], routes[1:2, :]
    epg = w_gate.shape[0]
    down = lax.broadcasted_iota(jnp.int32, (rows, rows), 0)
    across = lax.broadcasted_iota(jnp.int32, (rows, rows), 1)
    group = lax.broadcasted_iota(jnp.int32, (16, rows), 0)
    member = (first >= group * epg) & (first < group * epg + epg) & (group < GROUPS)
    member = jnp.where(member, 1.0, 0.0)
    earlier = jnp.where(down < across, 1.0, 0.0).astype(BF16)
    rank = dot(member.astype(BF16), earlier)
    slot = jnp.sum(member * (rank + (group * cap).astype(F32)), axis=0, keepdims=True)
    pick = jnp.where(slot == down.astype(F32), 1.0, 0.0)
    back = pick.T.astype(BF16)
    pick = pick.astype(BF16)
    low = jnp.where(first < second, route_weight[0:1, :], route_weight[1:2, :])
    high = jnp.where(first < second, route_weight[1:2, :], route_weight[0:1, :])
    low_top, high_top = low.astype(BF16).astype(F32), high.astype(BF16).astype(F32)
    line = lax.broadcasted_iota(jnp.int32, (LANES, rows), 0)
    scales = jnp.where(
        line == 0,
        low_top,
        jnp.where(
            line == 1,
            low - low_top,
            jnp.where(line == 2, high_top, jnp.where(line == 3, high - high_top, 0.0)),
        ),
    ).astype(BF16)
    scales = lax.dot_general(
        pick, scales, (((1,), (1,)), ((), ())), preferred_element_type=F32
    )
    weigh_out[...] = scales.astype(BF16)

    group_rows = lambda g: pl.ds(pl.multiple_of(g * cap, cap), cap)
    block = lambda place: pl.ds(pl.multiple_of(pos(place) * cap, cap), cap)

    def send_weigh(*others):
        for k in others:
            send(
                weigh_out.at[group_rows(sp_of[k]), :],
                weigh.at[s, block(t), :],
                WEIGH_SENT,
                weigh_recv.at[0],
                sp=sp_of[k],
            )

    @pl.when(middle)
    def _():
        send_weigh(1, 3)
        pl.semaphore_wait(known, 1)
        signal(known, sp=sp_of[1])
        send_weigh(2)

    @pl.when(s == 3)
    def _():
        pl.semaphore_wait(known, 2)
        send_weigh(1, 2, 3)

    @pl.when(s > 0)
    def _():
        wait_for(halo, halo_recv.at[0])
        gated[0:8, :] = halo[0, 8:16, :].astype(F32) * halo[1, 8:16, :].astype(F32)

    for i in range(3):

        @pl.when(partners[i] == 0)
        def _():
            mix_out[i, 0:edge, :] = mix(0, 0, edge)
            send_mixed(i, 0, edge)

    mix_in[t] = mix(t, 0, rows)


    weigh[s, block(t), :] = weigh_out[group_rows(s), :]

    def forward_weigh():
        wait_for(weigh.at[0:3, 0:cap, :], weigh_recv.at[0])
        for k in range(4):
            mine = weigh.at[sp_of[k], block(t), :]
            src = mine if k else weigh_out.at[group_rows(s), :]
            send(src, mine, WEIGH_SENT, weigh_recv.at[1], tp=chip)
            send(src, mine, WEIGH_SENT, weigh_recv.at[2], tp=core)

    def pass_weigh():
        wait_for(weigh.at[:, 0:cap, :], weigh_recv.at[1])
        for k in range(4):
            arrived = weigh.at[sp_of[k], block(chip), :]
            send(arrived, arrived, WEIGH_SENT, weigh_recv.at[2], tp=core)

    tile = 1024
    tiles = width // tile
    column = lambda n: pl.ds(pl.multiple_of(n * tile, tile), tile)
    weights_of = lambda place: pl.ds(pl.multiple_of(place * channels, channels), channels)
    loads[7].wait()
    loads[8].wait()
    wait_mixed(core)

    def project_near(n, carry):
        cols = column(n)
        total = residual[:, cols].astype(F32)
        for place in (t, core):
            total += dot(mix_in[place], proj[weights_of(place), cols])
        stream[:, cols] = total
        return carry

    lax.fori_loop(0, tiles, project_near, 0)

    @pl.when(s == 0)
    def _():
        pl.semaphore_wait(known, 2)
        send_weigh(1, 2, 3)

    sooner = far + (t % 2) * (chip - far)
    later = chip + far - sooner
    wait_mixed(sooner)

    def project_sooner(n, carry):
        cols = column(n)
        stream[:, cols] += dot(mix_in[sooner], proj[weights_of(sooner), cols])
        return carry

    lax.fori_loop(0, tiles, project_sooner, 0)
    wait_mixed(later)

    def project_later(n, squares):
        cols = column(n)
        total = stream[:, cols] + dot(mix_in[later], proj[weights_of(later), cols])
        stream[:, cols] = total
        return squares + jnp.sum(total * total, axis=1, keepdims=True)

    squares = lax.fori_loop(0, tiles, project_later, jnp.zeros((rows, 1), F32))
    scale = lax.rsqrt(squares / width + 1e-06)
    loads[6].wait()

    def forward(k, h):
        dst = tok.at[sp_of[k], h, block(t), :]
        src = leaving.at[h, group_rows(s), :]
        if k:
            wait_for(dst, z_recv.at[2 * k + h - 2])
            src = dst
        i = 2 * k + h
        send(src, dst, X_SENT, x_recv.at[i], tp=chip)
        send(src, dst, X_SENT, core_recv.at[i], tp=core)
        if not k:
            tok[s, h, block(t), :] = leaving[h, group_rows(s), :]

    def leave(k, h):
        send(
            leaving.at[h, group_rows(sp_of[k]), :],
            tok.at[s, h, block(t), :],
            Z_SENT,
            z_recv.at[2 * k + h - 2],
            sp=sp_of[k],
        )

    for h in (0, 1):

        def norm(n, carry):
            cols = column(n + h * (tiles // 2))
            row = (stream[:, cols] * scale * gain[:, cols]).astype(BF16)
            leaving[h, :, column(n)] = dot(pick, row).astype(BF16)
            return carry

        lax.fori_loop(0, tiles // 2, norm, 0)
        if h == 0:
            for stage in " ".join(EARLY).split():
                (leave if stage[0] == "Z" else forward)(*map(int, stage[1:]))

    for load in loads[9:]:
        load.wait()

    def pass_on(k, h):
        i = 2 * k + h
        arrived = tok.at[sp_of[k], h, block(chip), :]
        wait_for(arrived, x_recv.at[i])
        send(arrived, arrived, X_SENT, core_recv.at[i], tp=core)

    core_rows = lambda c: pl.ds(pl.multiple_of(c * 2 * cap, cap), 2 * cap)

    def experts(k, h):
        g = sp_of[k]
        wait_for(tok.at[g, h, 0 : 2 * cap, :], core_recv.at[2 * k + h])
        x = tok[g, h]
        deep = pl.ds(h * half, half)
        if h == 0:
            for e in range(epg):
                begun[k, 2 * e] = dot(x, w_gate[e, deep, :])
                begun[k, 2 * e + 1] = dot(x, w_up[e, deep, :])
            return
        top = weigh[g].astype(F32)
        for e in range(epg):
            w = top[:, 2 * e : 2 * e + 1] + top[:, 2 * e + 1 : 2 * e + 2]
            gate = begun[k, 2 * e] + dot(x, w_gate[e, deep, :])
            upper = begun[k, 2 * e + 1] + dot(x, w_up[e, deep, :])
            act = gate / (1.0 + jnp.exp(-gate)) * upper * w
            hidden[k, :, pl.ds(e * units, units)] = act.astype(BF16)

    def lower(k, h):
        def step(n, carry):
            cols = column(n + h * (tiles // 2))
            part[k, h, :, column(n)] = dot(hidden[k], w_down[:, cols]).astype(BF16)
            return carry

        lax.fori_loop(0, tiles // 2, step, 0)
        send(
            part.at[k, h, core_rows(1 - t % 2), :],
            from_core.at[k, h],
            ONE_SENT,
            one_recv.at[2 * k + h],
            tp=core,
        )

    def add_core(k, h):
        i = 2 * k + h
        wait_for(from_core.at[k, h], one_recv.at[i])
        for mine in (False, True):
            x = t // 2 if mine else 1 - t // 2
            base = pl.multiple_of((t % 2) * 2 * cap + x * cap, cap)
            near = pl.multiple_of(x * cap, cap)
            total = part[k, h, pl.ds(base, cap), :].astype(F32)
            total += from_core[k, h, pl.ds(near, cap), :].astype(F32)
            if mine:
                kept[k, h] = total
            else:
                to_chip[k, h] = total.astype(BF16)
                send(
                    to_chip.at[k, h],
                    from_chip.at[k, h],
                    TWO_SENT,
                    two_recv.at[i],
                    tp=chip,
                )

    def add_chip(k, h):
        wait_for(from_chip.at[k, h], two_recv.at[2 * k + h])
        total = (kept[k, h] + from_chip[k, h].astype(F32)).astype(BF16)
        if k == 0:
            home[h, group_rows(s), :] = total
        else:
            to_home[k, h] = total
            send(
                to_home.at[k, h],
                home.at[h, group_rows(s), :],
                Z_SENT,
                home_recv.at[h],
                sp=sp_of[k],
            )

    stages = dict(
        F=forward,
        P=pass_on,
        E=experts,
        L=lower,
        A=add_core,
        B=add_chip,
        W=forward_weigh,
        V=pass_weigh,
        Y=lambda: wait_for(weigh.at[:, 0 : 2 * cap, :], weigh_recv.at[2]),
        Z=leave,
    )
    for order in dict.fromkeys(ORDERS):
        where = [i for i in range(4) if ORDERS[i] == order]

        def run():
            for stage in " ".join(order).split():
                stages[stage[0]](*map(int, stage[1:]))

        if len(where) == 4:
            run()
        else:
            chosen = functools.reduce(jnp.logical_or, [s == i for i in where])
            pl.when(chosen)(run)

    for h in (0, 1):

        def finish(n, carry):
            cols = column(n + h * (tiles // 2))
            out[:, cols] = (stream[:, cols] + dot(back, home[h, :, column(n)])).astype(BF16)
            return carry

        wait_for(home.at[h, 0 : 3 * cap, :], home_recv.at[h])
        lax.fori_loop(0, tiles // 2, finish, 0)
    wait_for(tok.at[0:3], sent.at[X_SENT])
    wait_for(tok.at[0:3, :, 0 : 2 * cap, :], sent.at[Z_SENT])
    wait_for(tok.at[0:2], sent.at[ONE_SENT])
    wait_for(tok.at[0], sent.at[TWO_SENT])
    wait_for(mix_out, sent.at[MIX_SENT])
    wait_for(weigh.at[0:3], sent.at[WEIGH_SENT])
    wait_for(weigh.at[0:3, 0:cap, :], sent.at[WEIGH_SENT])

    @pl.when(s < 3)
    def _():
        wait_for(halo, sent.at[HALO_SENT])


def fused(*args):
    (conv_input, _, _, _, out_proj, residual, gain, _, _, w_gate, w_up, w_down) = args
    rows, width = residual.shape
    count, channels = conv_input.shape
    local, _, units = w_gate.shape
    cap = rows // GROUPS
    half = width // 2
    w_down = w_down.reshape(local * units, width)
    args = args[:6] + (gain.reshape(1, width), args[7].T, args[8].T) + args[9:11] + (w_down,)
    far = pl.BlockSpec(memory_space=pl.ANY)
    vmem, sems = pltpu.VMEM, pltpu.SemaphoreType.DMA
    return pl.pallas_call(
        fused_kernel,
        out_shape=vmem((rows, width), BF16),
        in_specs=[far] * 12,
        out_specs=pl.BlockSpec(memory_space=vmem),
        scratch_shapes=[vmem(arg.shape, arg.dtype) for arg in args]
        + [
            vmem((2, 16, channels), BF16),
            vmem((count + 8, channels), F32),
            vmem((3, rows, channels), BF16),
            vmem((4, rows, channels), BF16),
            vmem((rows, width), F32),
            vmem((rows, LANES), BF16),
            vmem((4, rows, LANES), BF16),
            vmem((2, rows, half), BF16),
            vmem((4, 2, rows, half), BF16),
            vmem((4, 2 * local, rows, units), F32),
            vmem((4, rows, local * units), BF16),
            vmem((4, 2, rows, half), BF16),
            vmem((4, 2, 2 * cap, half), BF16),
            vmem((4, 2, cap, half), F32),
            vmem((4, 2, cap, half), BF16),
            vmem((4, 2, cap, half), BF16),
            vmem((4, 2, cap, half), BF16),
            vmem((2, rows, half), BF16),
            pltpu.SemaphoreType.REGULAR,
        ]
        + [sems((n,)) for n in (12, 7, 1, 4, 3, 6, 8, 8, 8, 8, 2)],
        compiler_params=pltpu.CompilerParams(
            collective_id=0, has_side_effects=True, vmem_limit_bytes=56 << 20
        ),
    )(*args)


def on_device(*args):
    residual, routes, w_gate = args[5], args[7], args[9]
    rows, local, seq_ranks = residual.shape[0], w_gate.shape[0], lax.axis_size("sp")
    dense = local == routes.shape[1] == 2 and local * seq_ranks == local * GROUPS
    if dense and lax.axis_size("tp") == 4 and rows % LANES == 0:
        return fused(*args)
    return generic(*args)


def solution(mesh):
    return jax.shard_map(
        on_device,
        mesh=mesh,
        in_specs=(
            P(("grp", "sp"), "tp"),
            P(("grp", "sp"), "tp"),
            P(("grp", "sp"), "tp"),
            P(),
            P(),
            P(("grp", "sp", "tp"), None),
            P(),
            P(("grp", "sp", "tp"), None),
            P(("grp", "sp", "tp"), None),
            P("sp", None, "tp"),
            P("sp", None, "tp"),
            P("sp", "tp", None),
        ),
        out_specs=P(("grp", "sp", "tp"), None),
        check_vma=False,
    )
```
